32 devices in a mesh: grp: 2 (over x), ep: 8 (over z, y), tp: 2 (over core).
Axes of the slice: x: 2, y: 2, z: 4, core: 2. Of those that a mesh axis runs over, the one named last changes fastest.
Arguments:
- tokens: bfloat16 [1024, 2048], P(('grp', 'ep')), parts along dimension 0, may hold values from -6 to 6
- routes: int32 [1024, 4], P(('grp', 'ep')), parts along dimension 0, may hold values from 0 to 7, all different within a row; in each aligned block of 64 rows (0 to 63, 64 to 127, ...) at most 64 rows name the same one
- gate_weights: float32 [1024, 4], P(('grp', 'ep')), parts along dimension 0, may hold values from 0.05 to 1
- w_gate: bfloat16 [8, 2048, 1280], P('ep', None, 'tp'), may hold values from -0.125 to 0.125
- w_up: bfloat16 [8, 2048, 1280], P('ep', None, 'tp'), may hold values from -0.125 to 0.125
- w_down: bfloat16 [8, 1280, 2048], P('ep', 'tp'), may hold values from -0.15625 to 0.15625
- norm_gain: float32 [2048], P('tp'), may hold values from 0.1 to 1.9
- norm_bias: float32 [2048], P('tp'), may hold values from -2 to 2
Outputs:
- normed: bfloat16 [1024, 2048], P(('grp', 'ep'), 'tp'), parts along dimension 0
The draws below stay inside these ranges and needn't reach their ends.
There are 2 independent parts, one for each index of `grp`. The reference program is written for one: setup_inputs(seed, part) draws one part's arguments, and reference() takes and returns one part's arrays. A program takes and returns all parts, laid end to end along the dimension named above; an argument that names none is the same for every part. Nothing has to cross between parts.
Inputs may be any that keep to these rules, and one draw needn't show every extreme that they name: `routes`: the rows of a token name distinct experts; in each aligned block of 64 rows (the tokens of one index of ep) no expert is named more than 64 times, a bound that some block reaches.
All inputs are finite; a program needn't handle non-finite values.
Results may differ from the reference program's by a relative error of at most 0.0037.
Values may be sent and summed in bfloat16 or wider, within the bound.
No kernel may reach another device: no remote copies, remote signals or barrier semaphores. Data moves between devices by JAX's collectives and lax.ppermute only.
A program may use at most 64 MiB of HBM per device.

```python
import math
import jax
import jax.numpy as jnp
import numpy as np
from jax import lax

D = 2048
FF = 1280
TOP = 4
TOK_DEV = 64
EXPERTS = 8
CAP = 64
TOKENS = 512
N_EP = 8
N_TP = 2


def block_scale(key, extent, split, low, high):
    def one(position, blocks):
        draws = jax.random.uniform(jax.random.fold_in(jax.random.fold_in(key, 6), position), (blocks,), jnp.float32, low / len(split), high / len(split))
        return jnp.repeat(jnp.exp(draws), extent[position] // blocks).reshape((-1,) + (1,) * (len(extent) - position - 1))

    level = one(*split[0])
    for cut in split[1:]:
        level = level * one(*cut)
    return level


def routed_block(key, own, number, rows, count, top, reach, lean):
    sequence = jax.random.permutation(key, count)
    crowded, usual = portions_of(count, rows * top, reach, lean, True), portions_of(count, rows * top, reach, lean, False)
    places = jnp.arange(count)

    def named(lengths, rotation):
        used = int((lengths > 0).sum())
        fixed = max(1, used // 4)
        shifted = fixed + (places - fixed + rotation * (used - fixed)) % max(1, count - fixed)
        return jnp.zeros((count,), jnp.int32).at[sequence[jnp.where(places < fixed, places, shifted)]].set(jnp.asarray(lengths, jnp.int32))

    lengths = jnp.where(number % 4 == 0, named(crowded, number // 4), named(usual, number - number // 4 - 1))
    mixed = jax.random.permutation(jax.random.fold_in(own, 3), count)
    donor, taker = mixed[0:count // 2 * 2:2], mixed[1:count // 2 * 2:2]
    room = jnp.minimum(lengths[donor] - 1, reach - lengths[taker]) // 2
    room = jnp.where((donor == sequence[0]) | (taker == sequence[0]) | (lengths[taker] == 0), 0, jnp.maximum(room, 0))
    shifted = jax.random.randint(jax.random.fold_in(own, 4), (count // 2,), 0, 1 << 20) % (room + 1)
    lengths = lengths.at[donor].add(-shifted).at[taker].add(shifted)
    items = jnp.searchsorted(jnp.cumsum(lengths), jnp.arange(rows * top), side="right").astype(jnp.int32)
    grid = items.reshape(top, rows).T
    grid = grid[jax.random.permutation(jax.random.fold_in(own, 1), rows)]
    rotation = jax.random.randint(jax.random.fold_in(own, 2), (rows, 1), 0, top)
    return jnp.take_along_axis(grid, (jnp.arange(top)[None, :] + rotation) % top, axis=1)


def portions_of(amount, total, limit, skew, full):
    portions = [(1 << 20) // math.isqrt(rank ** skew) + 1 for rank in range(1, amount + 1)]
    largest = limit if full else min(limit, max(-(-total // amount), total * portions[0] // sum(portions)))
    least = 1 if total - largest >= amount - 1 else 0
    given, rest = [largest] + [least] * (amount - 1), total - largest - least * (amount - 1)
    while rest > 0:
        movable = [i for i in range(1, amount) if given[i] < largest] or [i for i in range(1, amount) if given[i] < limit]
        whole, left = sum([portions[i] for i in movable]), rest
        for i in movable:
            addition = min(limit - given[i], max(1, left * portions[i] // whole), rest)
            given[i] = given[i] + addition
            rest = rest - addition
    return np.array(given)


def gaussian(rng, dims, deviation, bound, pieces=(), kind=jnp.bfloat16):
    values = deviation * jax.random.normal(rng, dims, jnp.float32)
    if pieces:
        values = values * block_scale(rng, dims, pieces, -0.22, 0.18)
    return jnp.clip(values, -bound, bound).astype(kind)


def setup_inputs(seed: int = 0, part: int = 0) -> dict:
    streams_of = jax.random.split(jax.random.key(seed), 9)
    own_keys = jax.random.split(jax.random.fold_in(streams_of[8], part), 9)
    tokens = gaussian(own_keys[0], (TOKENS, D), 1.0, 6.0, ((0, 8),))
    routes_keys = jax.random.split(jax.random.fold_in(own_keys[1], 1), TOKENS // TOK_DEV)
    routes_turns = jax.random.permutation(jax.random.fold_in(own_keys[1], 3), TOKENS // TOK_DEV)
    routes = jax.vmap(lambda own, number: routed_block(jax.random.fold_in(own_keys[1], 2), own, number, TOK_DEV, EXPERTS, TOP, CAP, 2))(routes_keys, routes_turns).reshape((TOKENS, TOP))
    gate_weights = jnp.clip(jnp.exp(math.log(1.0) - 2.9957323 * jax.random.uniform(own_keys[2], (TOKENS, TOP), jnp.float32) ** block_scale(own_keys[2], (TOKENS, TOP), ((0, 8),), -0.2, 0.2)), 0.05, 1.0)
    w_gate = gaussian(streams_of[3], (EXPERTS, D, FF), D ** -0.5, 0.125, ((0, 8), (2, 2)))
    w_up = gaussian(streams_of[4], (EXPERTS, D, FF), D ** -0.5, 0.125, ((0, 8), (2, 2)))
    w_down = gaussian(streams_of[5], (EXPERTS, FF, D), FF ** -0.5, 0.15625, ((0, 8), (1, 2)))
    norm_gain = jnp.clip(1.0 + 0.18 * jax.random.normal(streams_of[6], (D,), jnp.float32), 0.1, 1.9)
    norm_bias = gaussian(streams_of[7], (D,), 0.4, 2.0, ((0, 2),), jnp.float32)
    return {"tokens": tokens, "routes": routes, "gate_weights": gate_weights, "w_gate": w_gate, "w_up": w_up, "w_down": w_down, "norm_gain": norm_gain, "norm_bias": norm_bias}


residual_scale = 1.4142135
norm_eps = 1e-05

def reference(tokens, routes, gate_weights, w_gate, w_up, w_down, norm_gain, norm_bias):
    pair_list = routes.reshape(N_EP, TOK_DEV * TOP).astype(jnp.int32)
    onehot = (pair_list[..., None] == jnp.arange(EXPERTS, dtype=jnp.int32)).astype(jnp.int32)
    slots = lax.optimization_barrier(jnp.sum((jnp.cumsum(onehot, axis=1) - onehot) * onehot, axis=-1))
    blocks = tokens.reshape(N_EP, TOK_DEV, D).astype(jnp.float32)
    weights = gate_weights.reshape(N_EP, TOK_DEV, TOP).astype(jnp.float32)
    columns = jnp.arange(CAP, dtype=jnp.int32)
    half = FF // N_TP

    def one_expert(carry, inputs):
        expert, gate_w, up_w, down_w = inputs
        picked = ((pair_list == expert)[..., None] & (slots[..., None] == columns)).astype(jnp.float32)
        picked = picked.reshape(N_EP, TOK_DEV, TOP, CAP)
        placed = lax.optimization_barrier(jnp.sum(picked, axis=2))
        rows = jnp.einsum('stc,std->scd', placed, blocks, precision=lax.Precision.HIGHEST)
        rows = rows.astype(jnp.bfloat16).reshape(N_EP * CAP, D)
        gate = jnp.dot(rows, gate_w, preferred_element_type=jnp.float32)
        upper = jnp.dot(rows, up_w, preferred_element_type=jnp.float32)
        hidden = (jax.nn.silu(gate) * upper).astype(jnp.bfloat16)
        total = jnp.zeros((N_EP * CAP, D), jnp.float32)
        for index in range(N_TP):
            partial_sum = jnp.dot(hidden[:, index * half:(index + 1) * half], down_w[index * half:(index + 1) * half], preferred_element_type=jnp.float32)
            total = total + lax.optimization_barrier(partial_sum.astype(jnp.bfloat16)).astype(jnp.float32)
        output = lax.optimization_barrier(total.astype(jnp.bfloat16)).astype(jnp.float32)
        output = output.reshape(N_EP, CAP, D)
        mixing = jnp.einsum('stkc,stk->stc', picked, weights, precision=lax.Precision.HIGHEST)
        carry = carry + jnp.einsum('stc,scd->std', mixing, output, precision=lax.Precision.HIGHEST)
        return (carry, None)
    start = jnp.zeros((N_EP, TOK_DEV, D), jnp.float32)
    mixed, _ = lax.scan(one_expert, start, (jnp.arange(EXPERTS, dtype=jnp.int32), w_gate, w_up, w_down))
    mixture = lax.optimization_barrier(mixed.reshape(TOKENS, D).astype(jnp.bfloat16)).astype(jnp.float32)
    summed = residual_scale * tokens.astype(jnp.float32) + mixture
    mean = lax.optimization_barrier(jnp.mean(summed, axis=-1, keepdims=True))
    variance = lax.optimization_barrier(jnp.mean(jnp.square(summed - mean), axis=-1, keepdims=True))
    normed = (summed - mean) * lax.rsqrt(variance + norm_eps) * norm_gain + norm_bias
    return normed.astype(jnp.bfloat16)
```

```python
import functools

import jax
import jax.numpy as jnp
from jax import lax
from jax.experimental import pallas as pl
from jax.experimental.pallas import tpu as pltpu
from jax.sharding import PartitionSpec as P

residual_scale = 1.4142135
norm_eps = 1e-05
LANES = 128


def by_slots(tokens, routes, gate_weights, w_gate, w_up, w_down, norm_gain, norm_bias):
    num_ep = lax.axis_size("ep")
    num_tp = lax.axis_size("tp")
    tp_index = lax.axis_index("tp")
    tok_rows, width = tokens.shape
    top_count = routes.shape[1]
    experts = num_ep * w_gate.shape[0]
    capacity = 2 * tok_rows * top_count // experts
    half_width = width // num_tp
    pair_list = routes.reshape(-1)
    onehot = (pair_list[:, None] == jnp.arange(experts, dtype=jnp.int32)).astype(jnp.int32)
    slots = jnp.sum((jnp.cumsum(onehot, axis=0) - onehot) * onehot, axis=1)
    target = pair_list * capacity + slots
    placing = jnp.arange(experts * capacity, dtype=jnp.int32)[:, None] == target[None, :]
    placing = jnp.sum(
        placing.reshape(experts * capacity, tok_rows, top_count).astype(jnp.float32), axis=2
    )
    placing = placing.astype(jnp.bfloat16)
    own_half = lax.dynamic_slice_in_dim(tokens, tp_index * half_width, half_width, 1)
    outgoing = jnp.dot(placing, own_half, preferred_element_type=jnp.float32).astype(jnp.bfloat16)
    arrived = lax.all_to_all(outgoing, "ep", split_axis=0, concat_axis=0, tiled=True)
    received = lax.all_gather(arrived, "tp", axis=1, tiled=True)
    gate = jnp.dot(received, w_gate[0], preferred_element_type=jnp.float32)
    upper = jnp.dot(received, w_up[0], preferred_element_type=jnp.float32)
    hidden = (jax.nn.silu(gate) * upper).astype(jnp.bfloat16)
    partial_sum = jnp.dot(hidden, w_down[0], preferred_element_type=jnp.float32).astype(
        jnp.bfloat16
    )
    expert_out = (
        lax.psum_scatter(partial_sum, "tp", scatter_dimension=1, tiled=True)
        .astype(jnp.float32)
        .astype(jnp.bfloat16)
    )
    came_back = lax.all_to_all(expert_out, "ep", split_axis=0, concat_axis=0, tiled=True)
    chosen = came_back[target].astype(jnp.float32).reshape(tok_rows, top_count, half_width)
    mixture = jnp.sum(gate_weights[:, :, None] * chosen, axis=1).astype(jnp.bfloat16)
    summed = residual_scale * own_half.astype(jnp.float32) + mixture.astype(jnp.float32)
    row_sum, row_squares = lax.psum(
        (jnp.sum(summed, axis=1), jnp.sum(summed * summed, axis=1)), "tp"
    )
    mean = row_sum / width
    variance = row_squares / width - mean * mean
    normed = (summed - mean[:, None]) * lax.rsqrt(
        variance[:, None] + norm_eps
    ) * norm_gain + norm_bias
    return normed.astype(jnp.bfloat16)


def expert_kernel(experts, width, kept, expert_ref, *refs):
    *row_refs, wg_ref, wu_ref, wd_ref, mine_ref, theirs_ref = refs
    packed = jnp.concatenate([r[...] for r in row_refs], axis=0)
    rows, codes = packed[:, :width], packed[:, width:].astype(jnp.float32)
    lane = lax.broadcasted_iota(jnp.int32, codes.shape, 1)
    named = (lane == expert_ref[0]) | (lane == expert_ref[0] + experts)
    weight = jnp.sum(jnp.where(named, codes, 0.0), axis=1, keepdims=True)
    ff = wg_ref.shape[1]
    step = 2 * LANES
    dot = functools.partial(jnp.dot, preferred_element_type=jnp.float32)
    hidden = []
    for start in range(0, ff - step + 1, step):
        gate = dot(rows, wg_ref[:, start : start + step])
        upper = dot(rows, wu_ref[:, start : start + step])
        hidden.append((jax.nn.silu(gate) * upper).astype(jnp.bfloat16))
    rest = ff % step
    if rest:
        both = dot(rows, jnp.concatenate([wg_ref[:, ff - rest :], wu_ref[:, ff - rest :]], axis=1))
        hidden.append((jax.nn.silu(both[:, :rest]) * both[:, rest:]).astype(jnp.bfloat16))
    hidden = jnp.concatenate(hidden, axis=1)
    for start in range(0, width, 2 * step):
        out = dot(hidden, wd_ref[:, start : start + 2 * step]) * weight
        mine_ref[:, start : start + 2 * step] = out[:kept]
        theirs_ref[:, start : start + 2 * step] = out[kept:].astype(jnp.bfloat16)


def run_expert(expert, experts, mine, theirs, w_gate, w_up, w_down):
    width = w_gate.shape[0]
    kept, sent = (sum(b.shape[0] for b in blocks) for blocks in (mine, theirs))
    vmem = pl.BlockSpec(memory_space=pltpu.VMEM)
    count = kept + sent
    flops = 6 * count * width * w_gate.shape[1]
    return pl.pallas_call(
        functools.partial(expert_kernel, experts, width, kept),
        out_shape=(
            jax.ShapeDtypeStruct((kept, width), jnp.float32),
            jax.ShapeDtypeStruct((sent, width), jnp.bfloat16),
        ),
        in_specs=[pl.BlockSpec(memory_space=pltpu.SMEM)] + [vmem] * (len(mine) + len(theirs) + 3),
        out_specs=(vmem, vmem),
        compiler_params=pltpu.CompilerParams(vmem_limit_bytes=40 << 20),
        cost_estimate=pl.CostEstimate(flops=flops, bytes_accessed=8 << 20, transcendentals=0),
        name="expert",
    )(expert, *mine, *theirs, w_gate, w_up, w_down)


def by_tokens(tokens, routes, gate_weights, w_gate, w_up, w_down, norm_gain, norm_bias):
    num_ep = lax.axis_size("ep")
    num_tp = lax.axis_size("tp")
    tp_index = lax.axis_index("tp")
    tok_rows, width = tokens.shape
    experts = num_ep * w_gate.shape[0]
    share = tok_rows // num_tp
    bf16, f32 = jnp.bfloat16, jnp.float32

    def over_ep(x, flip):
        return lax.ppermute(x, "ep", [(i, i ^ flip) for i in range(num_ep)])

    def over_tp(x):
        return lax.ppermute(x, "tp", [(i, i ^ 1) for i in range(num_tp)])

    ids = jnp.arange(experts, dtype=jnp.int32)
    scale = jnp.sum(
        jnp.where(routes[:, :, None] == ids, gate_weights[:, :, None], 0.0), axis=1
    )
    high = lax.reduce_precision(scale, 8, 7)
    codes = jnp.concatenate([high, scale - high], axis=1).astype(bf16)
    codes = jnp.pad(codes, ((0, 0), (0, -(2 * experts) % LANES)))
    packed = jnp.concatenate([tokens, codes], axis=1)
    own = lax.dynamic_slice_in_dim(packed, tp_index * share, share, 0)
    other = lax.dynamic_slice_in_dim(packed, (1 - tp_index) * share, share, 0)

    affine = jnp.stack([norm_gain, norm_bias])
    affine_other = over_tp(affine)

    far = range(1, num_ep // 2)
    got = {0: own} | {z: over_ep(own, 2 * z) for z in far}
    across = {z: over_ep(got[z], 1) for z in got}
    got_sib = {0: other} | {z: over_tp(got[z]) for z in far}
    across_sib = {z: over_tp(across[z]) for z in got}

    expert = lax.axis_index("ep").astype(jnp.int32).reshape(1)
    total = None
    for group in ((0, 1), *((z,) for z in range(2, num_ep // 2))):
        mine = [got[z] for z in group] + [across[z] for z in group]
        theirs = [got_sib[z] for z in group] + [across_sib[z] for z in group]
        kept, sent = run_expert(expert, experts, mine, theirs, w_gate[0], w_up[0], w_down[0])
        full = kept + over_tp(sent).astype(f32)
        rows = share * len(group)
        here = full[:rows] + over_ep(full[rows:].astype(bf16), 1).astype(f32)
        for i, z in enumerate(group):
            part = here[i * share : (i + 1) * share]
            if z:
                part = over_ep(part.astype(bf16), 2 * z).astype(f32)
            total = part if total is None else total + part
    mixture = total.astype(bf16).astype(f32)

    summed = residual_scale * own[:, :width].astype(f32) + mixture
    mean = jnp.mean(summed, axis=1, keepdims=True)
    centred = summed - mean
    variance = jnp.mean(centred * centred, axis=1, keepdims=True)
    first = tp_index == 0
    gain = jnp.concatenate(
        [jnp.where(first, affine, affine_other), jnp.where(first, affine_other, affine)], axis=1
    )
    normed = (centred * lax.rsqrt(variance + norm_eps) * gain[0] + gain[1]).astype(bf16)
    half = width // num_tp
    left, right = normed[:, :half], normed[:, half:]
    stay = jnp.where(first, left, right)
    swapped = over_tp(jnp.where(first, right, left))
    return jnp.concatenate(
        [jnp.where(first, stay, swapped), jnp.where(first, swapped, stay)], axis=0
    )


def shards(tokens, routes, gate_weights, w_gate, w_up, w_down, norm_gain, norm_bias):
    num_ep = lax.axis_size("ep")
    num_tp = lax.axis_size("tp")
    top_count = routes.shape[1]
    tok_rows = tokens.shape[0]
    experts = num_ep * w_gate.shape[0]
    slots = 2 * tok_rows * top_count
    few = num_ep * tok_rows <= slots and num_ep in (4, 8) and num_tp == 2 and experts == num_ep
    plan = by_tokens if few else by_slots
    return plan(tokens, routes, gate_weights, w_gate, w_up, w_down, norm_gain, norm_bias)


def solution(mesh):
    in_specs = (
        P(("grp", "ep"), None),
        P(("grp", "ep"), None),
        P(("grp", "ep"), None),
        P("ep", None, "tp"),
        P("ep", None, "tp"),
        P("ep", "tp", None),
        P("tp"),
        P("tp"),
    )
    out_specs = P(("grp", "ep"), "tp")
    return jax.shard_map(shards, mesh=mesh, in_specs=in_specs, out_specs=out_specs, check_vma=False)
```

```python
import functools

import jax
import jax.numpy as jnp
from jax import lax
from jax.experimental import pallas as pl
from jax.experimental.pallas import tpu as pltpu
from jax.sharding import PartitionSpec as P


residual_scale = 1.4142135
norm_eps = 1e-05
LANES = 128


def by_slots(tokens, routes, gate_weights, w_gate, w_up, w_down, norm_gain, norm_bias):
    num_ep = lax.axis_size("ep")
    num_tp = lax.axis_size("tp")
    tp_index = lax.axis_index("tp")
    tok_rows, width = tokens.shape
    top_count = routes.shape[1]
    experts = num_ep * w_gate.shape[0]
    capacity = 2 * tok_rows * top_count // experts
    half_width = width // num_tp
    pair_list = routes.reshape(-1)
    onehot = (pair_list[:, None] == jnp.arange(experts, dtype=jnp.int32)).astype(jnp.int32)
    slots = jnp.sum((jnp.cumsum(onehot, axis=0) - onehot) * onehot, axis=1)
    target = pair_list * capacity + slots
    placing = jnp.arange(experts * capacity, dtype=jnp.int32)[:, None] == target[None, :]
    placing = jnp.sum(
        placing.reshape(experts * capacity, tok_rows, top_count).astype(jnp.float32), axis=2
    )
    placing = placing.astype(jnp.bfloat16)
    own_half = lax.dynamic_slice_in_dim(tokens, tp_index * half_width, half_width, 1)
    outgoing = jnp.dot(placing, own_half, preferred_element_type=jnp.float32).astype(jnp.bfloat16)
    arrived = lax.all_to_all(outgoing, "ep", split_axis=0, concat_axis=0, tiled=True)
    received = lax.all_gather(arrived, "tp", axis=1, tiled=True)
    gate = jnp.dot(received, w_gate[0], preferred_element_type=jnp.float32)
    upper = jnp.dot(received, w_up[0], preferred_element_type=jnp.float32)
    hidden = (jax.nn.silu(gate) * upper).astype(jnp.bfloat16)
    partial_sum = jnp.dot(hidden, w_down[0], preferred_element_type=jnp.float32).astype(
        jnp.bfloat16
    )
    expert_out = (
        lax.psum_scatter(partial_sum, "tp", scatter_dimension=1, tiled=True)
        .astype(jnp.float32)
        .astype(jnp.bfloat16)
    )
    came_back = lax.all_to_all(expert_out, "ep", split_axis=0, concat_axis=0, tiled=True)
    chosen = came_back[target].astype(jnp.float32).reshape(tok_rows, top_count, half_width)
    mixture = jnp.sum(gate_weights[:, :, None] * chosen, axis=1).astype(jnp.bfloat16)
    summed = residual_scale * own_half.astype(jnp.float32) + mixture.astype(jnp.float32)
    row_sum, row_squares = lax.psum(
        (jnp.sum(summed, axis=1), jnp.sum(summed * summed, axis=1)), "tp"
    )
    mean = row_sum / width
    variance = row_squares / width - mean * mean
    normed = (summed - mean[:, None]) * lax.rsqrt(
        variance[:, None] + norm_eps
    ) * norm_gain + norm_bias
    return normed.astype(jnp.bfloat16)


VMEM = pl.BlockSpec(memory_space=pltpu.VMEM)
HBM = pl.BlockSpec(memory_space=pltpu.HBM)
ANY = pl.BlockSpec(memory_space=pl.ANY)
MIB = 1 << 20


def rows_kernel(experts, tokens_hbm, routes_hbm, gates_hbm, own_ref, other_ref, *scratch):
    tokens_ref, routes_ref, gates_ref, done = scratch
    pairs = ((routes_hbm, routes_ref), (gates_hbm, gates_ref), (tokens_hbm, tokens_ref))
    copies = [pltpu.make_async_copy(a, b, done.at[i]) for i, (a, b) in enumerate(pairs)]
    for copy in copies:
        copy.start()
    copies[0].wait()
    copies[1].wait()
    rows, width = tokens_ref.shape
    share = own_ref.shape[0]
    routes, gates = routes_ref[...], gates_ref[...]
    top = routes.shape[0]
    ids = lax.broadcasted_iota(jnp.int32, (experts, rows), 0)
    scale = jnp.zeros((experts, rows), jnp.float32)
    for k in range(top):
        scale += jnp.where(routes[k : k + 1] == ids, gates[k : k + 1], 0.0)
    high = scale.astype(jnp.bfloat16).astype(jnp.float32)
    spare = jnp.zeros((own_ref.shape[1] - width - 2 * experts, rows), jnp.float32)
    codes = jnp.concatenate([high, scale - high, spare], axis=0)
    codes = jnp.concatenate([codes, jnp.zeros((codes.shape[0], -rows % LANES), jnp.float32)], axis=1)
    codes = codes.T.astype(jnp.bfloat16)
    first = lax.axis_index("tp") == 0
    low, top_half = codes[:share], codes[share : 2 * share]
    own_ref[:, width:] = jnp.where(first, low, top_half)
    other_ref[:, width:] = jnp.where(first, top_half, low)
    copies[2].wait()
    low, top_half = tokens_ref[:share], tokens_ref[share:]
    own_ref[:, :width] = jnp.where(first, low, top_half)
    other_ref[:, :width] = jnp.where(first, top_half, low)


def expert_kernel(experts, width, kept, *refs):
    *row_refs, wg_ref, wu_ref, wd_ref, mine_ref, theirs_ref = refs
    packed = jnp.concatenate([r[...] for r in row_refs], axis=0)
    rows, codes = packed[:, :width], packed[:, width:].astype(jnp.float32)
    lane = lax.broadcasted_iota(jnp.int32, codes.shape, 1)
    expert = lax.axis_index("ep")
    named = (lane == expert) | (lane == expert + experts)
    weight = jnp.sum(jnp.where(named, codes, 0.0), axis=1, keepdims=True)
    ff = wg_ref.shape[1]
    step = 2 * LANES
    dot = functools.partial(jnp.dot, preferred_element_type=jnp.float32)
    hidden = []
    for start in range(0, ff - step + 1, step):
        gate = dot(rows, wg_ref[:, start : start + step])
        upper = dot(rows, wu_ref[:, start : start + step])
        hidden.append((jax.nn.silu(gate) * upper).astype(jnp.bfloat16))
    rest = ff % step
    if rest:
        both = dot(rows, jnp.concatenate([wg_ref[:, ff - rest :], wu_ref[:, ff - rest :]], axis=1))
        hidden.append((jax.nn.silu(both[:, :rest]) * both[:, rest:]).astype(jnp.bfloat16))
    hidden = jnp.concatenate(hidden, axis=1)
    for start in range(0, width, 2 * step):
        out = dot(hidden, wd_ref[:, start : start + 2 * step]) * weight
        mine_ref[:, start : start + 2 * step] = out[:kept]
        theirs_ref[:, start : start + 2 * step] = out[kept:].astype(jnp.bfloat16)


def run_expert(experts, mine, theirs, weights):
    width = weights[0].shape[0]
    kept, sent = (sum(b.shape[0] for b in blocks) for blocks in (mine, theirs))
    flops = 6 * (kept + sent) * width * weights[0].shape[1]
    return pl.pallas_call(
        functools.partial(expert_kernel, experts, width, kept),
        out_shape=(
            jax.ShapeDtypeStruct((kept, width), jnp.float32),
            jax.ShapeDtypeStruct((sent, width), jnp.bfloat16),
        ),
        in_specs=[VMEM] * (len(mine) + len(theirs) + 3),
        out_specs=(VMEM, VMEM),
        compiler_params=pltpu.CompilerParams(vmem_limit_bytes=24 * MIB),
        cost_estimate=pl.CostEstimate(flops=flops, bytes_accessed=8 * MIB, transcendentals=0),
        name="expert",
    )(*mine, *theirs, *weights)


PIECES = 4


def fetch_kernel(*refs):
    sources, targets, done = refs[:3], refs[4:7], refs[7]
    copies = []
    for i, (source, target) in enumerate(zip(sources, targets)):
        rows = source.shape[0] // PIECES
        for j in range(PIECES):
            part = pl.ds(j * rows, rows)
            copies.append(pltpu.make_async_copy(source.at[part], target.at[part], done.at[i, j]))
    for copy in copies:
        copy.start()
    for copy in copies:
        copy.wait()


def fetch(weights, after):
    return pl.pallas_call(
        fetch_kernel,
        out_shape=tuple(pltpu.VMEM(w.shape, w.dtype) for w in weights),
        in_specs=[HBM] * 3 + [ANY],
        out_specs=(VMEM,) * 3,
        scratch_shapes=[pltpu.SemaphoreType.DMA((3, PIECES))],
        compiler_params=pltpu.CompilerParams(vmem_limit_bytes=12 * MIB),
        cost_estimate=pl.CostEstimate(flops=1 << 30, bytes_accessed=8 * MIB, transcendentals=0),
        name="fetch",
    )(*(pltpu.with_memory_space_constraint(w, pltpu.HBM) for w in weights), after)


def small_call(body, out_shape, *operands):
    several = isinstance(out_shape, tuple)
    return pl.pallas_call(
        body,
        out_shape=out_shape,
        in_specs=[VMEM] * len(operands),
        out_specs=(VMEM,) * len(out_shape) if several else VMEM,
        compiler_params=pltpu.CompilerParams(vmem_limit_bytes=8 * MIB),
        cost_estimate=pl.CostEstimate(flops=1 << 26, bytes_accessed=MIB, transcendentals=0),
    )(*operands)


def join_kernel(kept_ref, came_ref, *out_refs):
    share = out_refs[0].shape[0]
    for i, out in enumerate(out_refs):
        part = pl.ds(i * share, share)
        out[...] = (kept_ref[part] + came_ref[part].astype(jnp.float32)).astype(out.dtype)


def add_kernel(kept_ref, came_ref, out_ref):
    total = kept_ref[...].astype(jnp.float32) + came_ref[...].astype(jnp.float32)
    out_ref[...] = total.astype(out_ref.dtype)


def norm_kernel(count, *refs):
    terms, (rows_ref, gain_ref, bias_ref, gain_other_ref, bias_other_ref), (stay_ref, go_ref) = (
        refs[:count],
        refs[count : count + 5],
        refs[count + 5 :],
    )
    half = stay_ref.shape[1]
    total = terms[0][...].astype(jnp.float32)
    for term in terms[1:]:
        total += term[...].astype(jnp.float32)
    mixture = total.astype(jnp.bfloat16).astype(jnp.float32)
    summed = residual_scale * rows_ref[:, : 2 * half].astype(jnp.float32) + mixture
    mean = jnp.mean(summed, axis=1, keepdims=True)
    centred = summed - mean
    variance = jnp.mean(centred * centred, axis=1, keepdims=True)
    unit = centred * lax.rsqrt(variance + norm_eps)
    first = lax.axis_index("tp") == 0
    left, right = unit[:, :half], unit[:, half:]
    stay = jnp.where(first, left, right) * gain_ref[...] + bias_ref[...]
    go = jnp.where(first, right, left) * gain_other_ref[...] + bias_other_ref[...]
    stay_ref[...] = stay.astype(jnp.bfloat16)
    go_ref[...] = go.astype(jnp.bfloat16)


def by_tokens(tokens, routes, gate_weights, w_gate, w_up, w_down, norm_gain, norm_bias):
    num_ep = lax.axis_size("ep")
    num_tp = lax.axis_size("tp")
    tok_rows, width = tokens.shape
    experts = num_ep * w_gate.shape[0]
    share = tok_rows // num_tp
    half = width // num_tp
    bf16, f32 = jnp.bfloat16, jnp.float32

    def over_ep(x, flip):
        return lax.ppermute(x, "ep", [(i, i ^ flip) for i in range(num_ep)])

    def over_tp(x):
        return lax.ppermute(x, "tp", [(i, i ^ 1) for i in range(num_tp)])

    packed = jax.ShapeDtypeStruct((share, width + 2 * experts + (-2 * experts) % LANES), bf16)
    sources = (tokens, routes.T, gate_weights.T)
    own, other = pl.pallas_call(
        functools.partial(rows_kernel, experts),
        out_shape=(packed, packed),
        in_specs=[HBM] * 3,
        out_specs=(VMEM, VMEM),
        scratch_shapes=[pltpu.VMEM(x.shape, x.dtype) for x in sources] + [pltpu.SemaphoreType.DMA((3,))],
        compiler_params=pltpu.CompilerParams(vmem_limit_bytes=8 * MIB),
        cost_estimate=pl.CostEstimate(flops=1 << 26, bytes_accessed=MIB, transcendentals=0),
        name="rows",
    )(*(pltpu.with_memory_space_constraint(x, pltpu.HBM) for x in sources))

    bits = flips(num_ep)
    rows = {0: own}
    for flip in bits:
        rows |= {r | flip: over_ep(rows[r], flip) for r in list(rows)}
    rows_sib = {0: other} | {r: over_tp(rows[r]) for r in range(1, num_ep)}
    affine = [norm_gain[None], norm_bias[None]]
    affine_other = [over_tp(a) for a in affine]
    weights = fetch((w_gate[0], w_up[0], w_down[0]), rows[bits[1]])

    sums = {}
    for group in groups(num_ep):
        kept, sent = run_expert(
            experts, [rows[r] for r in group], [rows_sib[r] for r in group], weights
        )
        came = over_tp(sent)
        kinds = tuple(jax.ShapeDtypeStruct((share, width), bf16 if r & 1 else f32) for r in group)
        sums |= dict(zip(group, small_call(join_kernel, kinds, kept, came)))
    terms = []
    for flip in reversed(bits):
        for r in sorted(sums, reverse=True):
            if r & flip:
                came = over_ep(sums.pop(r), flip)
                left = r ^ flip
                if left == 0:
                    terms.append(came)
                    continue
                sends = (left & -left) == flip * 2
                kind = jax.ShapeDtypeStruct((share, width), bf16 if sends else f32)
                sums[left] = small_call(add_kernel, kind, sums[left], came)
    terms.append(sums[0])
    out = jax.ShapeDtypeStruct((share, half), bf16)
    stay, go = small_call(functools.partial(norm_kernel, len(terms)), (out, out), *terms, own, *affine, *affine_other)
    came = over_tp(go)
    first = lax.axis_index("tp") == 0
    return jnp.concatenate([jnp.where(first, stay, came), jnp.where(first, came, stay)], axis=0)


def flips(num_ep):
    bits = []
    flip = num_ep // 2
    while flip:
        bits.append(flip)
        flip //= 2
    return bits


def groups(num_ep):
    far = num_ep // 2
    return [tuple(range(far))] + [(r, r + 1) for r in range(far, num_ep, 2)]


def shards(tokens, routes, gate_weights, w_gate, w_up, w_down, norm_gain, norm_bias):
    num_ep = lax.axis_size("ep")
    num_tp = lax.axis_size("tp")
    top_count = routes.shape[1]
    tok_rows = tokens.shape[0]
    experts = num_ep * w_gate.shape[0]
    slots = 2 * tok_rows * top_count
    few = num_ep * tok_rows <= slots and num_ep in (4, 8) and num_tp == 2 and experts == num_ep
    plan = by_tokens if few else by_slots
    return plan(tokens, routes, gate_weights, w_gate, w_up, w_down, norm_gain, norm_bias)


def solution(mesh):
    in_specs = (
        P(("grp", "ep"), None),
        P(("grp", "ep"), None),
        P(("grp", "ep"), None),
        P("ep", None, "tp"),
        P("ep", None, "tp"),
        P("ep", "tp", None),
        P("tp"),
        P("tp"),
    )
    out_specs = P(("grp", "ep"), "tp")
    return jax.shard_map(shards, mesh=mesh, in_specs=in_specs, out_specs=out_specs, check_vma=False)
```

```python
import functools

import jax
import jax.numpy as jnp
from jax import lax
from jax.experimental import pallas as pl
from jax.experimental.pallas import tpu as pltpu
from jax.sharding import PartitionSpec as P


residual_scale = 1.4142135
norm_eps = 1e-05
LANES = 128


def by_slots(tokens, routes, gate_weights, w_gate, w_up, w_down, norm_gain, norm_bias):
    num_ep = lax.axis_size("ep")
    num_tp = lax.axis_size("tp")
    tp_index = lax.axis_index("tp")
    tok_rows, width = tokens.shape
    top_count = routes.shape[1]
    experts = num_ep * w_gate.shape[0]
    capacity = 2 * tok_rows * top_count // experts
    half_width = width // num_tp
    pair_list = routes.reshape(-1)
    onehot = (pair_list[:, None] == jnp.arange(experts, dtype=jnp.int32)).astype(jnp.int32)
    slots = jnp.sum((jnp.cumsum(onehot, axis=0) - onehot) * onehot, axis=1)
    target = pair_list * capacity + slots
    placing = jnp.arange(experts * capacity, dtype=jnp.int32)[:, None] == target[None, :]
    placing = jnp.sum(
        placing.reshape(experts * capacity, tok_rows, top_count).astype(jnp.float32), axis=2
    )
    placing = placing.astype(jnp.bfloat16)
    own_half = lax.dynamic_slice_in_dim(tokens, tp_index * half_width, half_width, 1)
    outgoing = jnp.dot(placing, own_half, preferred_element_type=jnp.float32).astype(jnp.bfloat16)
    arrived = lax.all_to_all(outgoing, "ep", split_axis=0, concat_axis=0, tiled=True)
    received = lax.all_gather(arrived, "tp", axis=1, tiled=True)
    gate = jnp.dot(received, w_gate[0], preferred_element_type=jnp.float32)
    upper = jnp.dot(received, w_up[0], preferred_element_type=jnp.float32)
    hidden = (jax.nn.silu(gate) * upper).astype(jnp.bfloat16)
    partial_sum = jnp.dot(hidden, w_down[0], preferred_element_type=jnp.float32).astype(
        jnp.bfloat16
    )
    expert_out = (
        lax.psum_scatter(partial_sum, "tp", scatter_dimension=1, tiled=True)
        .astype(jnp.float32)
        .astype(jnp.bfloat16)
    )
    came_back = lax.all_to_all(expert_out, "ep", split_axis=0, concat_axis=0, tiled=True)
    chosen = came_back[target].astype(jnp.float32).reshape(tok_rows, top_count, half_width)
    mixture = jnp.sum(gate_weights[:, :, None] * chosen, axis=1).astype(jnp.bfloat16)
    summed = residual_scale * own_half.astype(jnp.float32) + mixture.astype(jnp.float32)
    row_sum, row_squares = lax.psum(
        (jnp.sum(summed, axis=1), jnp.sum(summed * summed, axis=1)), "tp"
    )
    mean = row_sum / width
    variance = row_squares / width - mean * mean
    normed = (summed - mean[:, None]) * lax.rsqrt(
        variance[:, None] + norm_eps
    ) * norm_gain + norm_bias
    return normed.astype(jnp.bfloat16)


VMEM = pl.BlockSpec(memory_space=pltpu.VMEM)
HBM = pl.BlockSpec(memory_space=pltpu.HBM)
ANY = pl.BlockSpec(memory_space=pl.ANY)
MIB = 1 << 20


def rows_kernel(experts, tokens_hbm, routes_hbm, gates_hbm, all_ref, own_ref, *scratch):
    tokens_ref, routes_ref, gates_ref, done = scratch
    pairs = ((routes_hbm, routes_ref), (gates_hbm, gates_ref), (tokens_hbm, tokens_ref))
    copies = [pltpu.make_async_copy(a, b, done.at[i]) for i, (a, b) in enumerate(pairs)]
    for copy in copies:
        copy.start()
    copies[0].wait()
    copies[1].wait()
    rows, width = tokens_ref.shape
    share = own_ref.shape[0]
    routes, gates = routes_ref[...], gates_ref[...]
    ids = lax.broadcasted_iota(jnp.int32, (experts, rows), 0)
    scale = jnp.zeros((experts, rows), jnp.float32)
    for k in range(routes.shape[0]):
        scale += jnp.where(routes[k : k + 1] == ids, gates[k : k + 1], 0.0)
    high = scale.astype(jnp.bfloat16).astype(jnp.float32)
    spare = jnp.zeros((own_ref.shape[1] - width - 2 * experts, rows), jnp.float32)
    codes = jnp.concatenate([high, scale - high, spare], axis=0)
    codes = jnp.concatenate([codes, jnp.zeros((codes.shape[0], -rows % LANES), jnp.float32)], axis=1)
    codes = codes.T[:rows].astype(jnp.bfloat16)
    first = lax.axis_index("tp") == 0
    own_ref[:, width:] = jnp.where(first, codes[:share], codes[share:])
    all_ref[:, width:] = codes
    copies[2].wait()
    own_ref[:, :width] = jnp.where(first, tokens_ref[:share], tokens_ref[share:])
    all_ref[:, :width] = tokens_ref[...]


def expert_kernel(experts, width, arrange, *refs):
    *row_refs, wg_ref, wu_ref, wd_ref, mine_ref, theirs_ref = refs
    kept = mine_ref.shape[0]
    packed = jnp.concatenate(arrange(*(r[...] for r in row_refs)), axis=0)
    rows, codes = packed[:, :width], packed[:, width:].astype(jnp.float32)
    lane = lax.broadcasted_iota(jnp.int32, codes.shape, 1)
    expert = lax.axis_index("ep")
    named = (lane == expert) | (lane == expert + experts)
    weight = jnp.sum(jnp.where(named, codes, 0.0), axis=1, keepdims=True)
    ff = wg_ref.shape[1]
    step = 2 * LANES
    dot = functools.partial(jnp.dot, preferred_element_type=jnp.float32)
    hidden = []
    for start in range(0, ff - step + 1, step):
        gate = dot(rows, wg_ref[:, start : start + step])
        upper = dot(rows, wu_ref[:, start : start + step])
        hidden.append((jax.nn.silu(gate) * upper).astype(jnp.bfloat16))
    rest = ff % step
    if rest:
        both = dot(rows, jnp.concatenate([wg_ref[:, ff - rest :], wu_ref[:, ff - rest :]], axis=1))
        hidden.append((jax.nn.silu(both[:, :rest]) * both[:, rest:]).astype(jnp.bfloat16))
    hidden = jnp.concatenate(hidden, axis=1)
    for start in range(0, width, 2 * step):
        out = dot(hidden, wd_ref[:, start : start + 2 * step]) * weight
        mine_ref[:, start : start + 2 * step] = out[:kept]
        theirs_ref[:, start : start + 2 * step] = out[kept:].astype(jnp.bfloat16)


def as_given(*blocks):
    return blocks


def near_blocks(own, came, other, across, across_other):
    first = lax.axis_index("tp") == 0
    pick = functools.partial(jnp.where, first)
    across = pick(across_other, across)
    return pick(own, came), pick(came, across), pick(other, own), pick(across, other)


def run_expert(experts, blocks, arrange, kept, weights):
    width = weights[0].shape[0]
    flops = 12 * kept * width * weights[0].shape[1]
    return pl.pallas_call(
        functools.partial(expert_kernel, experts, width, arrange),
        out_shape=(
            jax.ShapeDtypeStruct((kept, width), jnp.float32),
            jax.ShapeDtypeStruct((kept, width), jnp.bfloat16),
        ),
        in_specs=[VMEM] * (len(blocks) + 3),
        out_specs=(VMEM, VMEM),
        compiler_params=pltpu.CompilerParams(vmem_limit_bytes=24 * MIB),
        cost_estimate=pl.CostEstimate(flops=flops, bytes_accessed=8 * MIB, transcendentals=0),
        name="expert",
    )(*blocks, *weights)


PIECES = 4


def fetch_kernel(*refs):
    sources, targets, done = refs[:3], refs[4:7], refs[7]
    copies = []
    for i, (source, target) in enumerate(zip(sources, targets)):
        rows = source.shape[0] // PIECES
        for j in range(PIECES):
            part = pl.ds(j * rows, rows)
            copies.append(pltpu.make_async_copy(source.at[part], target.at[part], done.at[i, j]))
    for copy in copies:
        copy.start()
    for copy in copies:
        copy.wait()


def fetch(weights, after):
    return pl.pallas_call(
        fetch_kernel,
        out_shape=tuple(pltpu.VMEM(w.shape, w.dtype) for w in weights),
        in_specs=[HBM] * 3 + [ANY],
        out_specs=(VMEM,) * 3,
        scratch_shapes=[pltpu.SemaphoreType.DMA((3, PIECES))],
        compiler_params=pltpu.CompilerParams(vmem_limit_bytes=12 * MIB),
        cost_estimate=pl.CostEstimate(flops=1 << 30, bytes_accessed=8 * MIB, transcendentals=0),
        name="fetch",
    )(*(pltpu.with_memory_space_constraint(w, pltpu.HBM) for w in weights), after)


def small_call(body, out_shape, *operands):
    several = isinstance(out_shape, tuple)
    return pl.pallas_call(
        body,
        out_shape=out_shape,
        in_specs=[VMEM] * len(operands),
        out_specs=(VMEM,) * len(out_shape) if several else VMEM,
        compiler_params=pltpu.CompilerParams(vmem_limit_bytes=8 * MIB),
        cost_estimate=pl.CostEstimate(flops=1 << 26, bytes_accessed=MIB, transcendentals=0),
    )(*operands)


def join_kernel(kept_ref, came_ref, *out_refs):
    share = out_refs[0].shape[0]
    for i, out in enumerate(out_refs):
        part = pl.ds(i * share, share)
        out[...] = (kept_ref[part] + came_ref[part].astype(jnp.float32)).astype(out.dtype)


def add_kernel(kept_ref, came_ref, out_ref):
    total = kept_ref[...].astype(jnp.float32) + came_ref[...].astype(jnp.float32)
    out_ref[...] = total.astype(out_ref.dtype)


def cut_kernel(here_ref, came_ref, stay_ref, go_ref):
    share = stay_ref.shape[0]
    first = lax.axis_index("tp") == 0
    low, high = here_ref[...], came_ref[...]
    stay_ref[...] = jnp.where(first, low[:share], high[share:])
    go_ref[...] = jnp.where(first, low[share:], high[:share])


def norm_kernel(count, *refs):
    terms, (rows_ref, gain_ref, bias_ref, gain_other_ref, bias_other_ref), (stay_ref, go_ref) = (
        refs[:count],
        refs[count : count + 5],
        refs[count + 5 :],
    )
    half = stay_ref.shape[1]
    total = terms[0][...].astype(jnp.float32)
    for term in terms[1:]:
        total += term[...].astype(jnp.float32)
    mixture = total.astype(jnp.bfloat16).astype(jnp.float32)
    summed = residual_scale * rows_ref[:, : 2 * half].astype(jnp.float32) + mixture
    mean = jnp.mean(summed, axis=1, keepdims=True)
    centred = summed - mean
    variance = jnp.mean(centred * centred, axis=1, keepdims=True)
    unit = centred * lax.rsqrt(variance + norm_eps)
    first = lax.axis_index("tp") == 0
    left, right = unit[:, :half], unit[:, half:]
    stay = jnp.where(first, left, right) * gain_ref[...] + bias_ref[...]
    go = jnp.where(first, right, left) * gain_other_ref[...] + bias_other_ref[...]
    stay_ref[...] = stay.astype(jnp.bfloat16)
    go_ref[...] = go.astype(jnp.bfloat16)


def by_tokens(tokens, routes, gate_weights, w_gate, w_up, w_down, norm_gain, norm_bias):
    num_ep = lax.axis_size("ep")
    num_tp = lax.axis_size("tp")
    tok_rows, width = tokens.shape
    experts = num_ep * w_gate.shape[0]
    share = tok_rows // num_tp
    half = width // num_tp
    bf16, f32 = jnp.bfloat16, jnp.float32
    shape = jax.ShapeDtypeStruct

    def over_ep(x, flips):
        pairs = [
            (i * num_tp + c, (i ^ flips[c]) * num_tp + c)
            for i in range(num_ep)
            for c in range(num_tp)
            if flips[c] is not None
        ]
        return lax.ppermute(x, ("ep", "tp"), pairs)

    def over_tp(x, pairs=((0, 1), (1, 0))):
        return lax.ppermute(x, "tp", pairs)

    packed = width + 2 * experts + (-2 * experts) % LANES
    sources = (tokens, routes.T, gate_weights.T)
    full, own = pl.pallas_call(
        functools.partial(rows_kernel, experts),
        out_shape=(shape((tok_rows, packed), bf16), shape((share, packed), bf16)),
        in_specs=[HBM] * 3,
        out_specs=(VMEM, VMEM),
        scratch_shapes=[pltpu.VMEM(x.shape, x.dtype) for x in sources] + [pltpu.SemaphoreType.DMA((3,))],
        compiler_params=pltpu.CompilerParams(vmem_limit_bytes=8 * MIB),
        cost_estimate=pl.CostEstimate(flops=1 << 26, bytes_accessed=MIB, transcendentals=0),
        name="rows",
    )(*(pltpu.with_memory_space_constraint(x, pltpu.HBM) for x in sources))
    affine = [norm_gain[None], norm_bias[None]]
    affine_other = [over_tp(a) for a in affine]

    far = far_places(num_ep)
    near = over_ep(full, (1, 2))
    got = {z: over_ep(own, (2 * z, 2 * z)) for z in far}
    near_other = over_tp(near)
    near_across = over_ep(near, (None, 1))
    near_across_other = over_tp(near_across, ((1, 0),))
    weights = fetch((w_gate[0], w_up[0], w_down[0]), near)

    blocks = (full, near, near_other, near_across, near_across_other)
    kept, sent = run_expert(experts, blocks, near_blocks, 2 * tok_rows, weights)
    came = over_tp(sent)
    kinds = (shape((tok_rows, width), f32), shape((tok_rows, width), bf16))
    near_here, near_there = small_call(join_kernel, kinds, kept, came)
    here, there = {}, {}
    for z in far:
        across = over_ep(got[z], (1, 1))
        blocks = (got[z], across, over_tp(got[z]), over_tp(across))
        kept, sent = run_expert(experts, blocks, as_given, 2 * share, weights)
        came = over_tp(sent)
        kinds = (shape((share, width), f32), shape((share, width), bf16))
        here[z], there[z] = small_call(join_kernel, kinds, kept, came)

    came = over_ep(near_there, (1, 1))
    total = small_call(add_kernel, shape((tok_rows, width), bf16), near_here, came)
    came = over_ep(total, (None, 2))
    part = shape((share, width), bf16)
    stay, go = small_call(cut_kernel, (part, part), total, came)
    terms = [stay, over_tp(go)]
    for z in far:
        came = over_ep(there[z], (1, 1))
        total = small_call(add_kernel, shape((share, width), bf16), here[z], came)
        terms.append(over_ep(total, (2 * z, 2 * z)))

    out = shape((share, half), bf16)
    stay, go = small_call(
        functools.partial(norm_kernel, len(terms)), (out, out), *terms, own, *affine, *affine_other
    )
    came = over_tp(go)
    first = lax.axis_index("tp") == 0
    return jnp.concatenate([jnp.where(first, stay, came), jnp.where(first, came, stay)], axis=0)


def far_places(num_ep):
    return list(range(num_ep // 2 - 1, 1, -1))


def shards(tokens, routes, gate_weights, w_gate, w_up, w_down, norm_gain, norm_bias):
    num_ep = lax.axis_size("ep")
    num_tp = lax.axis_size("tp")
    top_count = routes.shape[1]
    tok_rows = tokens.shape[0]
    experts = num_ep * w_gate.shape[0]
    slots = 2 * tok_rows * top_count
    few = num_ep * tok_rows <= slots and num_ep in (4, 8) and num_tp == 2 and experts == num_ep
    plan = by_tokens if few else by_slots
    return plan(tokens, routes, gate_weights, w_gate, w_up, w_down, norm_gain, norm_bias)


def solution(mesh):
    in_specs = (
        P(("grp", "ep"), None),
        P(("grp", "ep"), None),
        P(("grp", "ep"), None),
        P("ep", None, "tp"),
        P("ep", None, "tp"),
        P("ep", "tp", None),
        P("tp"),
        P("tp"),
    )
    out_specs = P(("grp", "ep"), "tp")
    return jax.shard_map(shards, mesh=mesh, in_specs=in_specs, out_specs=out_specs, check_vma=False)
```

```python
import functools

import jax
import jax.numpy as jnp
from jax import lax
from jax.experimental import pallas as pl
from jax.experimental.pallas import tpu as pltpu
from jax.sharding import PartitionSpec as P


residual_scale = 1.4142135
norm_eps = 1e-05
LANES = 128


def by_slots(tokens, routes, gate_weights, w_gate, w_up, w_down, norm_gain, norm_bias):
    num_ep = lax.axis_size("ep")
    num_tp = lax.axis_size("tp")
    tp_index = lax.axis_index("tp")
    tok_rows, width = tokens.shape
    top_count = routes.shape[1]
    experts = num_ep * w_gate.shape[0]
    capacity = 2 * tok_rows * top_count // experts
    half_width = width // num_tp
    pair_list = routes.reshape(-1)
    onehot = (pair_list[:, None] == jnp.arange(experts, dtype=jnp.int32)).astype(jnp.int32)
    slots = jnp.sum((jnp.cumsum(onehot, axis=0) - onehot) * onehot, axis=1)
    target = pair_list * capacity + slots
    placing = jnp.arange(experts * capacity, dtype=jnp.int32)[:, None] == target[None, :]
    placing = jnp.sum(
        placing.reshape(experts * capacity, tok_rows, top_count).astype(jnp.float32), axis=2
    )
    placing = placing.astype(jnp.bfloat16)
    own_half = lax.dynamic_slice_in_dim(tokens, tp_index * half_width, half_width, 1)
    outgoing = jnp.dot(placing, own_half, preferred_element_type=jnp.float32).astype(jnp.bfloat16)
    arrived = lax.all_to_all(outgoing, "ep", split_axis=0, concat_axis=0, tiled=True)
    received = lax.all_gather(arrived, "tp", axis=1, tiled=True)
    gate = jnp.dot(received, w_gate[0], preferred_element_type=jnp.float32)
    upper = jnp.dot(received, w_up[0], preferred_element_type=jnp.float32)
    hidden = (jax.nn.silu(gate) * upper).astype(jnp.bfloat16)
    partial_sum = jnp.dot(hidden, w_down[0], preferred_element_type=jnp.float32).astype(
        jnp.bfloat16
    )
    expert_out = (
        lax.psum_scatter(partial_sum, "tp", scatter_dimension=1, tiled=True)
        .astype(jnp.float32)
        .astype(jnp.bfloat16)
    )
    came_back = lax.all_to_all(expert_out, "ep", split_axis=0, concat_axis=0, tiled=True)
    chosen = came_back[target].astype(jnp.float32).reshape(tok_rows, top_count, half_width)
    mixture = jnp.sum(gate_weights[:, :, None] * chosen, axis=1).astype(jnp.bfloat16)
    summed = residual_scale * own_half.astype(jnp.float32) + mixture.astype(jnp.float32)
    row_sum, row_squares = lax.psum(
        (jnp.sum(summed, axis=1), jnp.sum(summed * summed, axis=1)), "tp"
    )
    mean = row_sum / width
    variance = row_squares / width - mean * mean
    normed = (summed - mean[:, None]) * lax.rsqrt(
        variance[:, None] + norm_eps
    ) * norm_gain + norm_bias
    return normed.astype(jnp.bfloat16)


VMEM = pl.BlockSpec(memory_space=pltpu.VMEM)
HBM = pl.BlockSpec(memory_space=pltpu.HBM)
ANY = pl.BlockSpec(memory_space=pl.ANY)
MIB = 1 << 20


def rows_kernel(experts, tokens_hbm, routes_hbm, gates_hbm, all_ref, own_ref, *scratch):
    tokens_ref, routes_ref, gates_ref, done = scratch
    pairs = ((routes_hbm, routes_ref), (gates_hbm, gates_ref), (tokens_hbm, tokens_ref))
    copies = [pltpu.make_async_copy(a, b, done.at[i]) for i, (a, b) in enumerate(pairs)]
    for copy in copies:
        copy.start()
    copies[0].wait()
    copies[1].wait()
    rows, width = tokens_ref.shape
    share = own_ref.shape[0]
    routes, gates = routes_ref[...], gates_ref[...]
    ids = lax.broadcasted_iota(jnp.int32, (experts, rows), 0)
    scale = jnp.zeros((experts, rows), jnp.float32)
    for k in range(routes.shape[0]):
        scale += jnp.where(routes[k : k + 1] == ids, gates[k : k + 1], 0.0)
    high = scale.astype(jnp.bfloat16).astype(jnp.float32)
    spare = jnp.zeros((own_ref.shape[1] - width - 2 * experts, rows), jnp.float32)
    codes = jnp.concatenate([high, scale - high, spare], axis=0)
    codes = jnp.concatenate([codes, jnp.zeros((codes.shape[0], -rows % LANES), jnp.float32)], axis=1)
    codes = codes.T[:rows].astype(jnp.bfloat16)
    first = lax.axis_index("tp") == 0
    own_ref[:, width:] = jnp.where(first, codes[:share], codes[share:])
    all_ref[:, width:] = codes
    copies[2].wait()
    own_ref[:, :width] = jnp.where(first, tokens_ref[:share], tokens_ref[share:])
    all_ref[:, :width] = tokens_ref[...]


def expert_kernel(experts, width, arrange, *refs):
    *row_refs, wg_ref, wu_ref, wd_ref, mine_ref, theirs_ref = refs
    kept = mine_ref.shape[0]
    packed = jnp.concatenate(arrange(*(r[...] for r in row_refs)), axis=0)
    rows, codes = packed[:, :width], packed[:, width:].astype(jnp.float32)
    lane = lax.broadcasted_iota(jnp.int32, codes.shape, 1)
    expert = lax.axis_index("ep")
    named = (lane == expert) | (lane == expert + experts)
    weight = jnp.sum(jnp.where(named, codes, 0.0), axis=1, keepdims=True)
    ff = wg_ref.shape[1]
    step = 2 * LANES
    dot = functools.partial(jnp.dot, preferred_element_type=jnp.float32)
    hidden = []
    for start in range(0, ff - step + 1, step):
        gate = dot(rows, wg_ref[:, start : start + step])
        upper = dot(rows, wu_ref[:, start : start + step])
        hidden.append((jax.nn.silu(gate) * upper).astype(jnp.bfloat16))
    rest = ff % step
    if rest:
        both = dot(rows, jnp.concatenate([wg_ref[:, ff - rest :], wu_ref[:, ff - rest :]], axis=1))
        hidden.append((jax.nn.silu(both[:, :rest]) * both[:, rest:]).astype(jnp.bfloat16))
    hidden = jnp.concatenate(hidden, axis=1)
    for start in range(0, width, 2 * step):
        out = dot(hidden, wd_ref[:, start : start + 2 * step]) * weight
        mine_ref[:, start : start + 2 * step] = out[:kept]
        theirs_ref[:, start : start + 2 * step] = out[kept:].astype(jnp.bfloat16)


def as_given(*blocks):
    return blocks


def near_blocks(own, came, other, across, across_other):
    core = lax.axis_index("tp")
    first = core == 0
    share = own.shape[0] // 2
    pick = functools.partial(jnp.where, first)
    kinds = own, pick(other, came), pick(came, other), pick(across_other, across)
    low, high = [k[:share] for k in kinds], [k[share:] for k in kinds]
    return [pick(x, y) for x, y in zip(low + high, high + low)]


def run_expert(experts, blocks, arrange, kept, weights):
    width = weights[0].shape[0]
    flops = 12 * kept * width * weights[0].shape[1]
    return pl.pallas_call(
        functools.partial(expert_kernel, experts, width, arrange),
        out_shape=(
            jax.ShapeDtypeStruct((kept, width), jnp.float32),
            jax.ShapeDtypeStruct((kept, width), jnp.bfloat16),
        ),
        in_specs=[VMEM] * (len(blocks) + 3),
        out_specs=(VMEM, VMEM),
        compiler_params=pltpu.CompilerParams(vmem_limit_bytes=24 * MIB),
        cost_estimate=pl.CostEstimate(flops=flops, bytes_accessed=8 * MIB, transcendentals=0),
        name="expert",
    )(*blocks, *weights)


PIECES = 4


def fetch_kernel(*refs):
    sources, targets, done = refs[:3], refs[4:7], refs[7]
    copies = []
    for i, (source, target) in enumerate(zip(sources, targets)):
        rows = source.shape[0] // PIECES
        for j in range(PIECES):
            part = pl.ds(j * rows, rows)
            copies.append(pltpu.make_async_copy(source.at[part], target.at[part], done.at[i, j]))
    for copy in copies:
        copy.start()
    for copy in copies:
        copy.wait()


def fetch(weights, after):
    return pl.pallas_call(
        fetch_kernel,
        out_shape=tuple(pltpu.VMEM(w.shape, w.dtype) for w in weights),
        in_specs=[HBM] * 3 + [ANY],
        out_specs=(VMEM,) * 3,
        scratch_shapes=[pltpu.SemaphoreType.DMA((3, PIECES))],
        compiler_params=pltpu.CompilerParams(vmem_limit_bytes=12 * MIB),
        cost_estimate=pl.CostEstimate(flops=1 << 30, bytes_accessed=8 * MIB, transcendentals=0),
        name="fetch",
    )(*(pltpu.with_memory_space_constraint(w, pltpu.HBM) for w in weights), after)


def small_call(body, out_shape, *operands):
    several = isinstance(out_shape, tuple)
    return pl.pallas_call(
        body,
        out_shape=out_shape,
        in_specs=[VMEM] * len(operands),
        out_specs=(VMEM,) * len(out_shape) if several else VMEM,
        compiler_params=pltpu.CompilerParams(vmem_limit_bytes=8 * MIB),
        cost_estimate=pl.CostEstimate(flops=1 << 26, bytes_accessed=MIB, transcendentals=0),
    )(*operands)


def join_kernel(kept_ref, came_ref, *out_refs):
    share = out_refs[0].shape[0]
    for i, out in enumerate(out_refs):
        part = pl.ds(i * share, share)
        out[...] = (kept_ref[part] + came_ref[part].astype(jnp.float32)).astype(out.dtype)


def add_kernel(kept_ref, came_ref, out_ref):
    total = kept_ref[...].astype(jnp.float32) + came_ref[...].astype(jnp.float32)
    out_ref[...] = total.astype(out_ref.dtype)


def norm_kernel(count, *refs):
    terms, (rows_ref, gain_ref, bias_ref, gain_other_ref, bias_other_ref), (stay_ref, go_ref) = (
        refs[:count],
        refs[count : count + 5],
        refs[count + 5 :],
    )
    half = stay_ref.shape[1]
    total = terms[0][...].astype(jnp.float32)
    for term in terms[1:]:
        total += term[...].astype(jnp.float32)
    mixture = total.astype(jnp.bfloat16).astype(jnp.float32)
    summed = residual_scale * rows_ref[:, : 2 * half].astype(jnp.float32) + mixture
    mean = jnp.mean(summed, axis=1, keepdims=True)
    centred = summed - mean
    variance = jnp.mean(centred * centred, axis=1, keepdims=True)
    unit = centred * lax.rsqrt(variance + norm_eps)
    first = lax.axis_index("tp") == 0
    left, right = unit[:, :half], unit[:, half:]
    stay = jnp.where(first, left, right) * gain_ref[...] + bias_ref[...]
    go = jnp.where(first, right, left) * gain_other_ref[...] + bias_other_ref[...]
    stay_ref[...] = stay.astype(jnp.bfloat16)
    go_ref[...] = go.astype(jnp.bfloat16)


def by_tokens(tokens, routes, gate_weights, w_gate, w_up, w_down, norm_gain, norm_bias):
    num_ep = lax.axis_size("ep")
    num_tp = lax.axis_size("tp")
    tok_rows, width = tokens.shape
    experts = num_ep * w_gate.shape[0]
    share = tok_rows // num_tp
    half = width // num_tp
    bf16, f32 = jnp.bfloat16, jnp.float32
    shape = jax.ShapeDtypeStruct

    def over_ep(x, flips):
        pairs = [
            (i * num_tp + c, (i ^ flips[c]) * num_tp + c)
            for i in range(num_ep)
            for c in range(num_tp)
            if flips[c] is not None
        ]
        return lax.ppermute(x, ("ep", "tp"), pairs)

    def over_tp(x, pairs=((0, 1), (1, 0))):
        return lax.ppermute(x, "tp", pairs)

    packed = width + 2 * experts + (-2 * experts) % LANES
    sources = (tokens, routes.T, gate_weights.T)
    full, own = pl.pallas_call(
        functools.partial(rows_kernel, experts),
        out_shape=(shape((tok_rows, packed), bf16), shape((share, packed), bf16)),
        in_specs=[HBM] * 3,
        out_specs=(VMEM, VMEM),
        scratch_shapes=[pltpu.VMEM(x.shape, x.dtype) for x in sources] + [pltpu.SemaphoreType.DMA((3,))],
        compiler_params=pltpu.CompilerParams(vmem_limit_bytes=8 * MIB),
        cost_estimate=pl.CostEstimate(flops=1 << 26, bytes_accessed=MIB, transcendentals=0),
        name="rows",
    )(*(pltpu.with_memory_space_constraint(x, pltpu.HBM) for x in sources))
    affine = [norm_gain[None], norm_bias[None]]
    affine_other = [over_tp(a) for a in affine]

    far = far_places(num_ep)
    near = over_ep(full, (1, 2))
    got = {z: over_ep(own, (2 * z, 2 * z)) for z in far}
    near_other = over_tp(near)
    near_across = over_ep(near, (None, 1))
    near_across_other = over_tp(near_across, ((1, 0),))
    weights = fetch((w_gate[0], w_up[0], w_down[0]), near)

    blocks = (full, near, near_other, near_across, near_across_other)
    kept, sent = run_expert(experts, blocks, near_blocks, 2 * tok_rows, weights)
    came = over_tp(sent)
    kinds = (shape((tok_rows, width), f32), shape((tok_rows, width), bf16))
    near_here, near_there = small_call(join_kernel, kinds, kept, came)
    here, there = {}, {}
    for z in far:
        across = over_ep(got[z], (1, 1))
        blocks = (got[z], across, over_tp(got[z]), over_tp(across))
        kept, sent = run_expert(experts, blocks, as_given, 2 * share, weights)
        came = over_tp(sent)
        kinds = (shape((share, width), f32), shape((share, width), bf16))
        here[z], there[z] = small_call(join_kernel, kinds, kept, came)

    came = over_ep(near_there, (1, 1))
    kinds = (shape((share, width), f32), shape((share, width), bf16))
    total, go = small_call(join_kernel, kinds, near_here, came)
    terms = [total, over_ep(go, (2, 2))]
    for z in far:
        came = over_ep(there[z], (1, 1))
        total = small_call(add_kernel, shape((share, width), bf16), here[z], came)
        terms.append(over_ep(total, (2 * z, 2 * z)))

    out = shape((share, half), bf16)
    stay, go = small_call(
        functools.partial(norm_kernel, len(terms)), (out, out), *terms, own, *affine, *affine_other
    )
    came = over_tp(go)
    first = lax.axis_index("tp") == 0
    return jnp.concatenate([jnp.where(first, stay, came), jnp.where(first, came, stay)], axis=0)


def far_places(num_ep):
    return list(range(num_ep // 2 - 1, 1, -1))


def shards(tokens, routes, gate_weights, w_gate, w_up, w_down, norm_gain, norm_bias):
    num_ep = lax.axis_size("ep")
    num_tp = lax.axis_size("tp")
    top_count = routes.shape[1]
    tok_rows = tokens.shape[0]
    experts = num_ep * w_gate.shape[0]
    slots = 2 * tok_rows * top_count
    few = num_ep * tok_rows <= slots and num_ep in (4, 8) and num_tp == 2 and experts == num_ep
    plan = by_tokens if few else by_slots
    return plan(tokens, routes, gate_weights, w_gate, w_up, w_down, norm_gain, norm_bias)


def solution(mesh):
    in_specs = (
        P(("grp", "ep"), None),
        P(("grp", "ep"), None),
        P(("grp", "ep"), None),
        P("ep", None, "tp"),
        P("ep", None, "tp"),
        P("ep", "tp", None),
        P("tp"),
        P("tp"),
    )
    out_specs = P(("grp", "ep"), "tp")
    return jax.shard_map(shards, mesh=mesh, in_specs=in_specs, out_specs=out_specs, check_vma=False)
```

```python
import functools

import jax
import jax.numpy as jnp
from jax import lax
from jax.experimental import pallas as pl
from jax.experimental.pallas import tpu as pltpu
from jax.sharding import PartitionSpec as P


residual_scale = 1.4142135
norm_eps = 1e-05
LANES = 128


def by_slots(tokens, routes, gate_weights, w_gate, w_up, w_down, norm_gain, norm_bias):
    num_ep = lax.axis_size("ep")
    num_tp = lax.axis_size("tp")
    tp_index = lax.axis_index("tp")
    tok_rows, width = tokens.shape
    top_count = routes.shape[1]
    experts = num_ep * w_gate.shape[0]
    capacity = 2 * tok_rows * top_count // experts
    half_width = width // num_tp
    pair_list = routes.reshape(-1)
    onehot = (pair_list[:, None] == jnp.arange(experts, dtype=jnp.int32)).astype(jnp.int32)
    slots = jnp.sum((jnp.cumsum(onehot, axis=0) - onehot) * onehot, axis=1)
    target = pair_list * capacity + slots
    placing = jnp.arange(experts * capacity, dtype=jnp.int32)[:, None] == target[None, :]
    placing = jnp.sum(
        placing.reshape(experts * capacity, tok_rows, top_count).astype(jnp.float32), axis=2
    )
    placing = placing.astype(jnp.bfloat16)
    own_half = lax.dynamic_slice_in_dim(tokens, tp_index * half_width, half_width, 1)
    outgoing = jnp.dot(placing, own_half, preferred_element_type=jnp.float32).astype(jnp.bfloat16)
    arrived = lax.all_to_all(outgoing, "ep", split_axis=0, concat_axis=0, tiled=True)
    received = lax.all_gather(arrived, "tp", axis=1, tiled=True)
    gate = jnp.dot(received, w_gate[0], preferred_element_type=jnp.float32)
    upper = jnp.dot(received, w_up[0], preferred_element_type=jnp.float32)
    hidden = (jax.nn.silu(gate) * upper).astype(jnp.bfloat16)
    partial_sum = jnp.dot(hidden, w_down[0], preferred_element_type=jnp.float32).astype(
        jnp.bfloat16
    )
    expert_out = (
        lax.psum_scatter(partial_sum, "tp", scatter_dimension=1, tiled=True)
        .astype(jnp.float32)
        .astype(jnp.bfloat16)
    )
    came_back = lax.all_to_all(expert_out, "ep", split_axis=0, concat_axis=0, tiled=True)
    chosen = came_back[target].astype(jnp.float32).reshape(tok_rows, top_count, half_width)
    mixture = jnp.sum(gate_weights[:, :, None] * chosen, axis=1).astype(jnp.bfloat16)
    summed = residual_scale * own_half.astype(jnp.float32) + mixture.astype(jnp.float32)
    row_sum, row_squares = lax.psum(
        (jnp.sum(summed, axis=1), jnp.sum(summed * summed, axis=1)), "tp"
    )
    mean = row_sum / width
    variance = row_squares / width - mean * mean
    normed = (summed - mean[:, None]) * lax.rsqrt(
        variance[:, None] + norm_eps
    ) * norm_gain + norm_bias
    return normed.astype(jnp.bfloat16)


VMEM = pl.BlockSpec(memory_space=pltpu.VMEM)
HBM = pl.BlockSpec(memory_space=pltpu.HBM)
ANY = pl.BlockSpec(memory_space=pl.ANY)
MIB = 1 << 20


def rows_kernel(experts, tokens_hbm, routes_hbm, gates_hbm, all_ref, own_ref, *scratch):
    tokens_ref, routes_ref, gates_ref, done = scratch
    pairs = ((routes_hbm, routes_ref), (gates_hbm, gates_ref), (tokens_hbm, tokens_ref))
    copies = [pltpu.make_async_copy(a, b, done.at[i]) for i, (a, b) in enumerate(pairs)]
    for copy in copies:
        copy.start()
    copies[0].wait()
    copies[1].wait()
    rows, width = tokens_ref.shape
    share = own_ref.shape[0]
    routes, gates = routes_ref[...], gates_ref[...]
    ids = lax.broadcasted_iota(jnp.int32, (experts, rows), 0)
    scale = jnp.zeros((experts, rows), jnp.float32)
    for k in range(routes.shape[0]):
        scale += jnp.where(routes[k : k + 1] == ids, gates[k : k + 1], 0.0)
    high = scale.astype(jnp.bfloat16).astype(jnp.float32)
    spare = jnp.zeros((own_ref.shape[1] - width - 2 * experts, rows), jnp.float32)
    codes = jnp.concatenate([high, scale - high, spare], axis=0)
    codes = jnp.concatenate([codes, jnp.zeros((codes.shape[0], -rows % LANES), jnp.float32)], axis=1)
    codes = codes.T[:rows].astype(jnp.bfloat16)
    first = lax.axis_index("tp") == 0
    own_ref[:, width:] = jnp.where(first, codes[:share], codes[share:])
    all_ref[:, width:] = codes
    copies[2].wait()
    own_ref[:, :width] = jnp.where(first, tokens_ref[:share], tokens_ref[share:])
    all_ref[:, :width] = tokens_ref[...]


def expert_kernel(experts, width, arrange, blocks, extra, fetch, *refs):
    row_refs, extra_refs = refs[:blocks], refs[blocks : blocks + extra]
    blocks += extra
    sources = refs[blocks : blocks + 3]
    mine_ref, theirs_ref = refs[blocks + 3 : blocks + 5]
    wg_ref, wu_ref, wd_ref = refs[blocks + 5 : blocks + 8] if fetch else sources
    ff = wg_ref.shape[1]
    step, wide = 2 * LANES, 4 * LANES
    units = [(start, min(step, ff - start)) for start in range(0, ff, step)]
    copies = {}
    if fetch:
        done = refs[blocks + 8]

        def bring(which, start, size):
            part = pl.ds(start, size)
            source, target = sources[which].at[:, part], refs[blocks + 5 + which].at[:, part]
            copies[which, start] = pltpu.make_async_copy(source, target, done.at[len(copies)])

        for start, size in units:
            bring(0, start, size)
            bring(1, start, size)
        for start in range(0, width, wide):
            bring(2, start, wide)
        for copy in copies.values():
            copy.start()

    def ready(which, start):
        if fetch:
            copies[which, start].wait()

    kept = mine_ref.shape[0]
    packed = jnp.concatenate(arrange(*(r[...] for r in row_refs)), axis=0)
    rows, codes = packed[:, :width], packed[:, width:].astype(jnp.float32)
    lane = lax.broadcasted_iota(jnp.int32, codes.shape, 1)
    expert = lax.axis_index("ep")
    named = (lane == expert) | (lane == expert + experts)
    weight = jnp.sum(jnp.where(named, codes, 0.0), axis=1, keepdims=True)
    dot = functools.partial(jnp.dot, preferred_element_type=jnp.float32)
    hidden = []
    for start, size in units:
        ready(0, start)
        if size == step:
            gate = dot(rows, wg_ref[:, start : start + size])
            ready(1, start)
            upper = dot(rows, wu_ref[:, start : start + size])
        else:
            ready(1, start)
            both = jnp.concatenate([wg_ref[:, start:], wu_ref[:, start:]], axis=1)
            both = dot(rows, both)
            gate, upper = both[:, :size], both[:, size:]
        hidden.append((jax.nn.silu(gate) * upper).astype(jnp.bfloat16))
    hidden = jnp.concatenate(hidden, axis=1)
    for start in range(0, width, wide):
        ready(2, start)
        out = dot(hidden, wd_ref[:, start : start + wide]) * weight
        mine_ref[:, start : start + wide] = out[:kept]
        theirs_ref[:kept, start : start + wide] = out[kept:].astype(jnp.bfloat16)
    for ref in extra_refs:
        theirs_ref[kept:] = ref[...]


def as_given(*blocks):
    return blocks


def halves(*blocks):
    first = lax.axis_index("tp") == 0
    share = blocks[0].shape[0] // 2
    low, high = [k[:share] for k in blocks], [k[share:] for k in blocks]
    return [jnp.where(first, x, y) for x, y in zip(low + high, high + low)]


def own_and_y(own, came, other):
    return halves(own, jnp.where(lax.axis_index("tp") == 0, came, other))


def z_and_zy(came, other, across, across_other):
    first = lax.axis_index("tp") == 0
    mine, theirs = halves(jnp.where(first, other, came))
    return mine, across, theirs, across_other


def run_expert(experts, blocks, arrange, kept, weights, fetch=False, also=None):
    width, ff = weights[0].shape
    flops = 12 * kept * width * ff
    out_shape = [
        jax.ShapeDtypeStruct((kept, width), jnp.float32),
        jax.ShapeDtypeStruct((kept if also is None else kept + also.shape[0], width), jnp.bfloat16),
    ]
    scratch = []
    extra = [] if also is None else [also]
    if fetch:
        weights = [pltpu.with_memory_space_constraint(w, pltpu.HBM) for w in weights]
        out_shape += [pltpu.VMEM(w.shape, w.dtype) for w in weights]
        pieces = 2 * -(-ff // (2 * LANES)) + width // (4 * LANES)
        scratch = [pltpu.SemaphoreType.DMA((pieces,))]
    return pl.pallas_call(
        functools.partial(expert_kernel, experts, width, arrange, len(blocks), len(extra), fetch),
        out_shape=tuple(out_shape),
        in_specs=[VMEM] * len(blocks + tuple(extra)) + [HBM if fetch else VMEM] * 3,
        out_specs=(VMEM,) * len(out_shape),
        scratch_shapes=scratch,
        compiler_params=pltpu.CompilerParams(vmem_limit_bytes=24 * MIB),
        cost_estimate=pl.CostEstimate(flops=flops, bytes_accessed=8 * MIB, transcendentals=0),
        name="expert",
    )(*blocks, *extra, *weights)


def small_call(body, out_shape, *operands, flops=1 << 26, moved=MIB):
    several = isinstance(out_shape, tuple)
    return pl.pallas_call(
        body,
        out_shape=out_shape,
        in_specs=[VMEM] * len(operands),
        out_specs=(VMEM,) * len(out_shape) if several else VMEM,
        compiler_params=pltpu.CompilerParams(vmem_limit_bytes=8 * MIB),
        cost_estimate=pl.CostEstimate(flops=flops, bytes_accessed=moved, transcendentals=0),
    )(*operands)


def share_kernel(block_ref, out_ref):
    share = out_ref.shape[0]
    out_ref[...] = jnp.where(lax.axis_index("tp") == 0, block_ref[:share], block_ref[share:])


def near_kernel(kept_ref, near_kept_ref, came_ref, there_ref, here_ref):
    rows = there_ref.shape[0]
    came = came_ref[...].astype(jnp.float32)
    there_ref[...] = (kept_ref[...] + came[:rows]).astype(jnp.bfloat16)
    here_ref[...] = near_kept_ref[...] + came[rows:]


def join_kernel(inputs, *refs):
    start = 0
    for out in refs[inputs:]:
        part = pl.ds(start, out.shape[0])
        total = refs[0][part].astype(jnp.float32)
        for ref in refs[1:inputs]:
            total += ref[part].astype(jnp.float32)
        out[...] = total.astype(out.dtype)
        start += out.shape[0]


def join(out_shape, *terms):
    return small_call(functools.partial(join_kernel, len(terms)), out_shape, *terms)


def norm_kernel(count, *refs):
    terms, (rows_ref, gain_ref, bias_ref, gain_other_ref, bias_other_ref), (stay_ref, go_ref) = (
        refs[:count],
        refs[count : count + 5],
        refs[count + 5 :],
    )
    half = stay_ref.shape[1]
    total = terms[0][...].astype(jnp.float32)
    for term in terms[1:]:
        total += term[...].astype(jnp.float32)
    mixture = total.astype(jnp.bfloat16).astype(jnp.float32)
    summed = residual_scale * rows_ref[:, : 2 * half].astype(jnp.float32) + mixture
    mean = jnp.mean(summed, axis=1, keepdims=True)
    centred = summed - mean
    variance = jnp.mean(centred * centred, axis=1, keepdims=True)
    unit = centred * lax.rsqrt(variance + norm_eps)
    first = lax.axis_index("tp") == 0
    left, right = unit[:, :half], unit[:, half:]
    stay = jnp.where(first, left, right) * gain_ref[...] + bias_ref[...]
    go = jnp.where(first, right, left) * gain_other_ref[...] + bias_other_ref[...]
    stay_ref[...] = stay.astype(jnp.bfloat16)
    go_ref[...] = go.astype(jnp.bfloat16)


def by_tokens(tokens, routes, gate_weights, w_gate, w_up, w_down, norm_gain, norm_bias):
    num_ep = lax.axis_size("ep")
    num_tp = lax.axis_size("tp")
    tok_rows, width = tokens.shape
    experts = num_ep * w_gate.shape[0]
    share = tok_rows // num_tp
    half = width // num_tp
    bf16, f32 = jnp.bfloat16, jnp.float32
    shape = jax.ShapeDtypeStruct

    def over_ep(x, flips):
        pairs = [
            (i * num_tp + c, (i ^ flips[c]) * num_tp + c)
            for i in range(num_ep)
            for c in range(num_tp)
            if flips[c] is not None
        ]
        return lax.ppermute(x, ("ep", "tp"), pairs)

    def over_tp(x, pairs=((0, 1), (1, 0))):
        return lax.ppermute(x, "tp", pairs)

    packed = width + 2 * experts + (-2 * experts) % LANES
    sources = (tokens, routes.T, gate_weights.T)
    full, own = pl.pallas_call(
        functools.partial(rows_kernel, experts),
        out_shape=(shape((tok_rows, packed), bf16), shape((share, packed), bf16)),
        in_specs=[HBM] * 3,
        out_specs=(VMEM, VMEM),
        scratch_shapes=[pltpu.VMEM(x.shape, x.dtype) for x in sources] + [pltpu.SemaphoreType.DMA((3,))],
        compiler_params=pltpu.CompilerParams(vmem_limit_bytes=8 * MIB),
        cost_estimate=pl.CostEstimate(flops=1<<34, bytes_accessed=MIB, transcendentals=0),
        name="rows",
    )(*(pltpu.with_memory_space_constraint(x, pltpu.HBM) for x in sources))
    affine = [norm_gain[None], norm_bias[None]]
    affine_other = [over_tp(a) for a in affine]

    far = far_places(num_ep)
    near = over_ep(full, (1, 2))
    got = {z: over_ep(own, (2 * z, 2 * z)) for z in far}
    near_other = over_tp(near)
    near_own = small_call(share_kernel, shape((share, packed), bf16), near, flops=1<<34, moved=MIB)
    near_across = over_ep(near_own, (2, 1))
    near_across_other = over_tp(near_across)

    weights = w_gate[0], w_up[0], w_down[0]
    kept, sent = run_expert(experts, (full, near, near_other), own_and_y, tok_rows, weights)
    near_kept = kept
    blocks = (near, near_other, near_across, near_across_other)
    kept, sent = run_expert(experts, blocks, z_and_zy, tok_rows, weights, also=sent)
    came = over_tp(sent)
    kinds = (shape((tok_rows, width), bf16), shape((tok_rows, width), f32))
    near_there, near_here = small_call(near_kernel, kinds, kept, near_kept, came)
    here, there = {}, {}
    for z in far:
        across = over_ep(got[z], (1, 1))
        blocks = (got[z], across, over_tp(got[z]), over_tp(across))
        kept, sent = run_expert(experts, blocks, as_given, 2 * share, weights)
        came = over_tp(sent)
        kinds = (shape((share, width), f32), shape((share, width), bf16))
        here[z], there[z] = join(kinds, kept, came)

    came = over_ep(near_there, (2, 2))
    kinds = (shape((share, width), f32), shape((share, width), bf16))
    total, go = join(kinds, near_here, came)
    terms = [total, over_ep(go, (1, 1))]
    for z in far:
        came = over_ep(there[z], (1, 1))
        total = join(shape((share, width), bf16), here[z], came)
        terms.append(over_ep(total, (2 * z, 2 * z)))

    out = shape((share, half), bf16)
    stay, go = small_call(functools.partial(norm_kernel, len(terms)), (out, out), *terms, own, *affine, *affine_other)
    came = over_tp(go)
    first = lax.axis_index("tp") == 0
    return jnp.concatenate([jnp.where(first, stay, came), jnp.where(first, came, stay)], axis=0)


def far_places(num_ep):
    return list(range(num_ep // 2 - 1, 1, -1))


def shards(tokens, routes, gate_weights, w_gate, w_up, w_down, norm_gain, norm_bias):
    num_ep = lax.axis_size("ep")
    num_tp = lax.axis_size("tp")
    top_count = routes.shape[1]
    tok_rows = tokens.shape[0]
    experts = num_ep * w_gate.shape[0]
    slots = 2 * tok_rows * top_count
    few = num_ep * tok_rows <= slots and num_ep in (4, 8) and num_tp == 2 and experts == num_ep
    plan = by_tokens if few else by_slots
    return plan(tokens, routes, gate_weights, w_gate, w_up, w_down, norm_gain, norm_bias)


def solution(mesh):
    in_specs = (
        P(("grp", "ep"), None),
        P(("grp", "ep"), None),
        P(("grp", "ep"), None),
        P("ep", None, "tp"),
        P("ep", None, "tp"),
        P("ep", "tp", None),
        P("tp"),
        P("tp"),
    )
    out_specs = P(("grp", "ep"), "tp")
    return jax.shard_map(shards, mesh=mesh, in_specs=in_specs, out_specs=out_specs, check_vma=False)
```

```python
import functools

import jax
import jax.numpy as jnp
from jax import lax
from jax.experimental import pallas as pl
from jax.experimental.pallas import tpu as pltpu
from jax.sharding import PartitionSpec as P


residual_scale = 1.4142135
norm_eps = 1e-05
LANES = 128


def by_slots(tokens, routes, gate_weights, w_gate, w_up, w_down, norm_gain, norm_bias):
    num_ep = lax.axis_size("ep")
    num_tp = lax.axis_size("tp")
    tp_index = lax.axis_index("tp")
    tok_rows, width = tokens.shape
    top_count = routes.shape[1]
    experts = num_ep * w_gate.shape[0]
    capacity = 2 * tok_rows * top_count // experts
    half_width = width // num_tp
    pair_list = routes.reshape(-1)
    onehot = (pair_list[:, None] == jnp.arange(experts, dtype=jnp.int32)).astype(jnp.int32)
    slots = jnp.sum((jnp.cumsum(onehot, axis=0) - onehot) * onehot, axis=1)
    target = pair_list * capacity + slots
    placing = jnp.arange(experts * capacity, dtype=jnp.int32)[:, None] == target[None, :]
    placing = jnp.sum(
        placing.reshape(experts * capacity, tok_rows, top_count).astype(jnp.float32), axis=2
    )
    placing = placing.astype(jnp.bfloat16)
    own_half = lax.dynamic_slice_in_dim(tokens, tp_index * half_width, half_width, 1)
    outgoing = jnp.dot(placing, own_half, preferred_element_type=jnp.float32).astype(jnp.bfloat16)
    arrived = lax.all_to_all(outgoing, "ep", split_axis=0, concat_axis=0, tiled=True)
    received = lax.all_gather(arrived, "tp", axis=1, tiled=True)
    gate = jnp.dot(received, w_gate[0], preferred_element_type=jnp.float32)
    upper = jnp.dot(received, w_up[0], preferred_element_type=jnp.float32)
    hidden = (jax.nn.silu(gate) * upper).astype(jnp.bfloat16)
    partial_sum = jnp.dot(hidden, w_down[0], preferred_element_type=jnp.float32).astype(
        jnp.bfloat16
    )
    expert_out = (
        lax.psum_scatter(partial_sum, "tp", scatter_dimension=1, tiled=True)
        .astype(jnp.float32)
        .astype(jnp.bfloat16)
    )
    came_back = lax.all_to_all(expert_out, "ep", split_axis=0, concat_axis=0, tiled=True)
    chosen = came_back[target].astype(jnp.float32).reshape(tok_rows, top_count, half_width)
    mixture = jnp.sum(gate_weights[:, :, None] * chosen, axis=1).astype(jnp.bfloat16)
    summed = residual_scale * own_half.astype(jnp.float32) + mixture.astype(jnp.float32)
    row_sum, row_squares = lax.psum(
        (jnp.sum(summed, axis=1), jnp.sum(summed * summed, axis=1)), "tp"
    )
    mean = row_sum / width
    variance = row_squares / width - mean * mean
    normed = (summed - mean[:, None]) * lax.rsqrt(
        variance[:, None] + norm_eps
    ) * norm_gain + norm_bias
    return normed.astype(jnp.bfloat16)


VMEM = pl.BlockSpec(memory_space=pltpu.VMEM)
HBM = pl.BlockSpec(memory_space=pltpu.HBM)
ANY = pl.BlockSpec(memory_space=pl.ANY)
MIB = 1 << 20


def rows_kernel(experts, tokens_hbm, routes_hbm, gates_hbm, all_ref, own_ref, *scratch):
    tokens_ref, routes_ref, gates_ref, done = scratch
    pairs = ((routes_hbm, routes_ref), (gates_hbm, gates_ref), (tokens_hbm, tokens_ref))
    copies = [pltpu.make_async_copy(a, b, done.at[i]) for i, (a, b) in enumerate(pairs)]
    for copy in copies:
        copy.start()
    copies[0].wait()
    copies[1].wait()
    rows, width = tokens_ref.shape
    share = own_ref.shape[0]
    routes, gates = routes_ref[...], gates_ref[...]
    ids = lax.broadcasted_iota(jnp.int32, (experts, rows), 0)
    scale = jnp.zeros((experts, rows), jnp.float32)
    for k in range(routes.shape[0]):
        scale += jnp.where(routes[k : k + 1] == ids, gates[k : k + 1], 0.0)
    high = scale.astype(jnp.bfloat16).astype(jnp.float32)
    spare = jnp.zeros((own_ref.shape[1] - width - 2 * experts, rows), jnp.float32)
    codes = jnp.concatenate([high, scale - high, spare], axis=0)
    codes = jnp.concatenate([codes, jnp.zeros((codes.shape[0], -rows % LANES), jnp.float32)], axis=1)
    codes = codes.T[:rows].astype(jnp.bfloat16)
    first = lax.axis_index("tp") == 0
    own_ref[:, width:] = jnp.where(first, codes[:share], codes[share:])
    all_ref[:, width:] = codes
    copies[2].wait()
    own_ref[:, :width] = jnp.where(first, tokens_ref[:share], tokens_ref[share:])
    all_ref[:, :width] = tokens_ref[...]


def expert_kernel(experts, width, arrange, blocks, *refs):
    row_refs, (wg_ref, wu_ref, wd_ref) = refs[:blocks], refs[blocks : blocks + 3]
    *extra_refs, mine_ref, theirs_ref = refs[blocks + 3 :]
    wide = 4 * LANES
    kept = mine_ref.shape[0]
    packed = jnp.concatenate(arrange(*(r[...] for r in row_refs)), axis=0)
    rows, codes = packed[:, :width], packed[:, width:].astype(jnp.float32)
    lane = lax.broadcasted_iota(jnp.int32, codes.shape, 1)
    expert = lax.axis_index("ep")
    named = (lane == expert) | (lane == expert + experts)
    weight = jnp.sum(jnp.where(named, codes, 0.0), axis=1, keepdims=True)
    dot = functools.partial(jnp.dot, preferred_element_type=jnp.float32)
    gate, upper = dot(rows, wg_ref[...]), dot(rows, wu_ref[...])
    hidden = (jax.nn.silu(gate) * upper).astype(jnp.bfloat16)
    for start in range(0, width, wide):
        out = dot(hidden, wd_ref[:, start : start + wide]) * weight
        mine_ref[:, start : start + wide] = out[:kept]
        theirs_ref[:kept, start : start + wide] = out[kept:].astype(jnp.bfloat16)
    for ref in extra_refs:
        theirs_ref[kept:] = ref[...]


def as_given(*blocks):
    return blocks


def halves(*blocks):
    first = lax.axis_index("tp") == 0
    share = blocks[0].shape[0] // 2
    low, high = [k[:share] for k in blocks], [k[share:] for k in blocks]
    return [jnp.where(first, x, y) for x, y in zip(low + high, high + low)]


def own_and_y(own, came, other):
    return halves(own, jnp.where(lax.axis_index("tp") == 0, came, other))


def z_and_zy(came, other, across, across_other):
    first = lax.axis_index("tp") == 0
    mine, theirs = halves(jnp.where(first, other, came))
    return mine, across, theirs, across_other


def run_expert(experts, blocks, arrange, kept, weights, *extra):
    width, ff = weights[0].shape
    sent = kept + sum(x.shape[0] for x in extra)
    return pl.pallas_call(
        functools.partial(expert_kernel, experts, width, arrange, len(blocks)),
        out_shape=(
            jax.ShapeDtypeStruct((kept, width), jnp.float32),
            jax.ShapeDtypeStruct((sent, width), jnp.bfloat16),
        ),
        in_specs=[VMEM] * (len(blocks) + 3 + len(extra)),
        out_specs=(VMEM, VMEM),
        compiler_params=pltpu.CompilerParams(vmem_limit_bytes=24 * MIB),
        cost_estimate=pl.CostEstimate(
            flops=12 * kept * width * ff, bytes_accessed=8 * MIB, transcendentals=0
        ),
        name="expert",
    )(*blocks, *weights, *extra)


def small_call(body, out_shape, *operands, flops=1 << 26, moved=MIB):
    several = isinstance(out_shape, tuple)
    return pl.pallas_call(
        body,
        out_shape=out_shape,
        in_specs=[VMEM] * len(operands),
        out_specs=(VMEM,) * len(out_shape) if several else VMEM,
        compiler_params=pltpu.CompilerParams(vmem_limit_bytes=8 * MIB),
        cost_estimate=pl.CostEstimate(flops=flops, bytes_accessed=moved, transcendentals=0),
    )(*operands)


def near_kernel(kept_ref, near_kept_ref, came_ref, there_ref, here_ref):
    rows = there_ref.shape[0]
    came = came_ref[...].astype(jnp.float32)
    there_ref[...] = (kept_ref[...] + came[:rows]).astype(jnp.bfloat16)
    here_ref[...] = near_kept_ref[...] + came[rows:]


def join_kernel(inputs, *refs):
    start = 0
    for out in refs[inputs:]:
        part = pl.ds(start, out.shape[0])
        total = refs[0][part].astype(jnp.float32)
        for ref in refs[1:inputs]:
            total += ref[part].astype(jnp.float32)
        out[...] = total.astype(out.dtype)
        start += out.shape[0]


def join(out_shape, *terms):
    return small_call(functools.partial(join_kernel, len(terms)), out_shape, *terms)


def norm_kernel(count, *refs):
    terms, (rows_ref, gain_ref, bias_ref, gain_other_ref, bias_other_ref), (stay_ref, go_ref) = (
        refs[:count],
        refs[count : count + 5],
        refs[count + 5 :],
    )
    half = stay_ref.shape[1]
    total = terms[0][...].astype(jnp.float32)
    for term in terms[1:]:
        total += term[...].astype(jnp.float32)
    mixture = total.astype(jnp.bfloat16).astype(jnp.float32)
    summed = residual_scale * rows_ref[:, : 2 * half].astype(jnp.float32) + mixture
    mean = jnp.mean(summed, axis=1, keepdims=True)
    centred = summed - mean
    variance = jnp.mean(centred * centred, axis=1, keepdims=True)
    unit = centred * lax.rsqrt(variance + norm_eps)
    first = lax.axis_index("tp") == 0
    left, right = unit[:, :half], unit[:, half:]
    stay = jnp.where(first, left, right) * gain_ref[...] + bias_ref[...]
    go = jnp.where(first, right, left) * gain_other_ref[...] + bias_other_ref[...]
    stay_ref[...] = stay.astype(jnp.bfloat16)
    go_ref[...] = go.astype(jnp.bfloat16)


def by_tokens(tokens, routes, gate_weights, w_gate, w_up, w_down, norm_gain, norm_bias):
    num_ep = lax.axis_size("ep")
    num_tp = lax.axis_size("tp")
    tok_rows, width = tokens.shape
    experts = num_ep * w_gate.shape[0]
    share = tok_rows // num_tp
    half = width // num_tp
    bf16, f32 = jnp.bfloat16, jnp.float32
    shape = jax.ShapeDtypeStruct

    def over_ep(x, flips):
        pairs = [
            (i * num_tp + c, (i ^ flips[c]) * num_tp + c)
            for i in range(num_ep)
            for c in range(num_tp)
            if flips[c] is not None
        ]
        return lax.ppermute(x, ("ep", "tp"), pairs)

    def over_tp(x, pairs=((0, 1), (1, 0))):
        return lax.ppermute(x, "tp", pairs)

    packed = width + 2 * experts + (-2 * experts) % LANES
    sources = (tokens, routes.T, gate_weights.T)
    full, own = pl.pallas_call(
        functools.partial(rows_kernel, experts),
        out_shape=(shape((tok_rows, packed), bf16), shape((share, packed), bf16)),
        in_specs=[HBM] * 3,
        out_specs=(VMEM, VMEM),
        scratch_shapes=[pltpu.VMEM(x.shape, x.dtype) for x in sources] + [pltpu.SemaphoreType.DMA((3,))],
        compiler_params=pltpu.CompilerParams(vmem_limit_bytes=8 * MIB),
        cost_estimate=pl.CostEstimate(flops=1<<34, bytes_accessed=MIB, transcendentals=0),
        name="rows",
    )(*(pltpu.with_memory_space_constraint(x, pltpu.HBM) for x in sources))
    affine = [norm_gain[None], norm_bias[None]]
    affine_other = [over_tp(a) for a in affine]

    far = far_places(num_ep)
    near = over_ep(full, (1, 2))
    got = {z: over_ep(own, (2 * z, 2 * z)) for z in far}
    near_other = over_tp(near)
    near_across = over_ep(own, (3, 3))
    near_across_other = over_tp(near_across)

    weights = w_gate[0], w_up[0], w_down[0]
    kept, sent = run_expert(experts, (full, near, near_other), own_and_y, tok_rows, weights)
    near_kept = kept
    blocks = (near, near_other, near_across, near_across_other)
    kept, sent = run_expert(experts, blocks, z_and_zy, tok_rows, weights, sent)
    came = over_tp(sent)
    kinds = (shape((tok_rows, width), bf16), shape((tok_rows, width), f32))
    near_there, near_here = small_call(near_kernel, kinds, kept, near_kept, came)
    here, there = {}, {}
    for z in far:
        across = over_ep(got[z], (1, 1))
        blocks = (got[z], across, over_tp(got[z]), over_tp(across))
        kept, sent = run_expert(experts, blocks, as_given, 2 * share, weights)
        came = over_tp(sent)
        kinds = (shape((share, width), f32), shape((share, width), bf16))
        here[z], there[z] = join(kinds, kept, came)

    came = over_ep(near_there, (2, 2))
    kinds = (shape((share, width), f32), shape((share, width), bf16))
    total, go = join(kinds, near_here, came)
    terms = [total, over_ep(go, (1, 1))]
    for z in far:
        came = over_ep(there[z], (1, 1))
        total = join(shape((share, width), bf16), here[z], came)
        terms.append(over_ep(total, (2 * z, 2 * z)))

    out = shape((share, half), bf16)
    stay, go = small_call(
        functools.partial(norm_kernel, len(terms)), (out, out), *terms, own, *affine, *affine_other
    )
    came = over_tp(go)
    first = lax.axis_index("tp") == 0
    return jnp.concatenate([jnp.where(first, stay, came), jnp.where(first, came, stay)], axis=0)


def far_places(num_ep):
    return list(range(num_ep // 2 - 1, 1, -1))


def shards(tokens, routes, gate_weights, w_gate, w_up, w_down, norm_gain, norm_bias):
    num_ep = lax.axis_size("ep")
    num_tp = lax.axis_size("tp")
    top_count = routes.shape[1]
    tok_rows = tokens.shape[0]
    experts = num_ep * w_gate.shape[0]
    slots = 2 * tok_rows * top_count
    few = num_ep * tok_rows <= slots and num_ep in (4, 8) and num_tp == 2 and experts == num_ep
    plan = by_tokens if few else by_slots
    return plan(tokens, routes, gate_weights, w_gate, w_up, w_down, norm_gain, norm_bias)


def solution(mesh):
    in_specs = (
        P(("grp", "ep"), None),
        P(("grp", "ep"), None),
        P(("grp", "ep"), None),
        P("ep", None, "tp"),
        P("ep", None, "tp"),
        P("ep", "tp", None),
        P("tp"),
        P("tp"),
    )
    out_specs = P(("grp", "ep"), "tp")
    return jax.shard_map(shards, mesh=mesh, in_specs=in_specs, out_specs=out_specs, check_vma=False)
```
